32 devices in a mesh: sp: 4 (over y, x), dp: 8 (over z, core).
Axes of the slice: x: 2, y: 2, z: 4, core: 2. Of those that a mesh axis runs over, the one named last changes fastest.
Arguments:
- tokens: bfloat16 [8, 512, 2048], P('dp', 'sp'), may hold values from -6 to 6
- query_weight: bfloat16 [2048, 1024], P('dp'), may hold values from -0.125 to 0.125
- key_weight: bfloat16 [2048, 1024], P('dp'), may hold values from -0.125 to 0.125
- value_weight: bfloat16 [2048, 2048], P('dp'), may hold values from -0.125 to 0.125
- output_weight: bfloat16 [2048, 2048], P('dp'), may hold values from -0.125 to 0.125
- log_decay: float32 [2, 16], P(None, 'sp'), may hold values from -0.04 to 0, as said below
Outputs:
- mixed: bfloat16 [8, 512, 2048], P('dp', 'sp')
The draws below stay inside these ranges and needn't reach their ends.
Inputs may be any that keep to these rules, and one draw needn't show every extreme that they name: `log_decay`: every entry is negative: the logarithm of a head's decay per position.
All inputs are finite; a program needn't handle non-finite values.
Results may differ from the reference program's by a relative error of at most 0.012.
Values may be sent and summed in bfloat16 or wider, within the bound.
A program may use at most 128 MiB of HBM per device.

```python
import jax
import jax.numpy as jnp
from jax import lax

D = 2048
HEADS = 16
DK = 64
DV = 128
BLOCK = 512
SEQ = 512
SEQS = 8


def draw_log_decay(key, part):
    first_key, second_key, third_key = jax.random.split(jax.random.fold_in(key, 17), 3)
    share = 0.5
    fast = jax.random.uniform(first_key, (2, HEADS), jnp.float32) < share
    fast_rate = jnp.exp(jax.random.uniform(second_key, (2, HEADS), jnp.float32, jnp.log(1.0 / 80.0), jnp.log(1.0 / 25.0)))
    slow_rate = jax.random.uniform(third_key, (2, HEADS), jnp.float32, 0.3, 2.0) / SEQ
    return (-jnp.where(fast, fast_rate, slow_rate)).astype(jnp.float32)


def level_of(rng, dims, shards, smallest, largest):
    factor_of, own = 1.0, jax.random.fold_in(rng, 6)
    for axis_at, shards_of in shards:
        draws = jnp.exp(jax.random.uniform(jax.random.fold_in(own, axis_at), (shards_of,), jnp.float32, smallest / len(shards), largest / len(shards)))
        factor_of = factor_of * jnp.repeat(draws, dims[axis_at] // shards_of).reshape([-1 if axis == axis_at else 1 for axis in range(len(dims))])
    return factor_of


def gaussian(key, extent, deviation, bound, cuts=(), kind=jnp.bfloat16):
    values = deviation * jax.random.normal(key, extent, jnp.float32)
    if cuts:
        values = values * level_of(key, extent, cuts, -0.22, 0.18)
    return jnp.clip(values, -bound, bound).astype(kind)


def setup_inputs(seed: int = 0) -> dict:
    splits = jax.random.split(jax.random.key(seed), 7)
    return {
        "tokens": gaussian(splits[0], (SEQS, SEQ, D), 1.0, 6.0, ((0, 8), (1, 4))),
        "query_weight": gaussian(splits[1], (D, HEADS * DK), D ** -0.5, 0.125, ((0, 8),)),
        "key_weight": gaussian(splits[2], (D, HEADS * DK), D ** -0.5, 0.125, ((0, 8),)),
        "value_weight": gaussian(splits[3], (D, HEADS * DV), D ** -0.5, 0.125, ((0, 8),)),
        "output_weight": gaussian(splits[4], (HEADS * DV, D), (HEADS * DV) ** -0.5, 0.125, ((0, 8),)),
        "log_decay": draw_log_decay(jax.random.fold_in(splits[6], 71), 0),
    }


exact_precision = lax.Precision.HIGHEST

def rotate(values_part, positions):
    half_dim = values_part.shape[-1] // 2
    frequency = 10000.0 ** (-jnp.arange(half_dim, dtype=jnp.float32) / half_dim)
    angles = positions[:, None] * frequency[None, :]
    cosine = jnp.cos(angles)[:, None, :]
    sine_part = jnp.sin(angles)[:, None, :]
    first = values_part[..., :half_dim]
    second = values_part[..., half_dim:]
    return jnp.concatenate([first * cosine - second * sine_part, first * sine_part + second * cosine], axis=-1)

def retain(query, key_rows, value_rows, log_rate):
    length, heads, key_dim = query.shape
    value_dim = value_rows.shape[-1]
    count = length // BLOCK
    offsets = jnp.arange(BLOCK, dtype=jnp.float32)
    distance = offsets[:, None] - offsets[None, :]
    decay_inner = jnp.where(distance[None] >= 0.0, jnp.exp(log_rate[:, None, None] * jnp.maximum(distance, 0.0)[None]), 0.0)
    decay_query = jnp.exp((offsets[:, None] + 1.0) * log_rate[None, :])[:, :, None]
    decay_key = jnp.exp((BLOCK - 1.0 - offsets)[:, None] * log_rate[None, :])[:, :, None]
    decay_block = jnp.exp(BLOCK * log_rate)[:, None, None]

    def blocks(array):
        return array.reshape(count, BLOCK, heads, array.shape[-1])

    def advance(state, inputs):
        query_block, key_block, value_block = inputs
        query_wide = query_block.astype(jnp.float32)
        key_wide = key_block.astype(jnp.float32)
        value_wide = value_block.astype(jnp.float32)
        inner = jnp.einsum('ihd,jhd->hij', query_wide, key_wide, precision=exact_precision) * decay_inner
        inner = inner.astype(jnp.bfloat16).astype(jnp.float32)
        result = jnp.einsum('hij,jhv->ihv', inner, value_wide, precision=exact_precision)
        result = result + jnp.einsum('ihd,hdv->ihv', query_wide * decay_query, state, precision=exact_precision)
        state = state * decay_block + jnp.einsum('jhd,jhv->hdv', key_wide * decay_key, value_wide, precision=exact_precision)
        return (state, result)
    initial = jnp.zeros((heads, key_dim, value_dim), jnp.float32)
    final_state, outputs = lax.scan(advance, initial, (blocks(query), blocks(key_rows), blocks(value_rows)))
    return outputs.reshape(length, heads, value_dim)

def mechanism(stacked, log_decay):
    length = stacked.shape[0]
    widened = stacked[..., :2 * DK].astype(jnp.float32)
    positions = jnp.arange(length, dtype=jnp.float32)
    query = rotate(widened[..., :DK], positions).astype(jnp.bfloat16)
    key_rows = rotate(widened[..., DK:2 * DK], positions).astype(jnp.bfloat16)
    value_rows = stacked[..., 2 * DK:]
    forward = retain(query, key_rows, value_rows, log_decay[0])
    backward = retain(jnp.flip(query, 0), jnp.flip(key_rows, 0), jnp.flip(value_rows, 0), log_decay[1])
    combined = forward + jnp.flip(backward, 0)
    average = lax.optimization_barrier(jnp.mean(combined, axis=-1, keepdims=True))
    centred = combined - average
    variance = lax.optimization_barrier(jnp.mean(centred * centred, axis=-1, keepdims=True))
    return (centred * lax.rsqrt(variance + 1e-06)).astype(jnp.bfloat16)

def reference(tokens, query_weight, key_weight, value_weight, output_weight, log_decay):

    def one_sequence(rows):
        length = rows.shape[0]
        query = jnp.dot(rows, query_weight, preferred_element_type=jnp.float32).astype(jnp.bfloat16).reshape(length, HEADS, DK)
        key_rows = jnp.dot(rows, key_weight, preferred_element_type=jnp.float32).astype(jnp.bfloat16).reshape(length, HEADS, DK)
        value_rows = jnp.dot(rows, value_weight, preferred_element_type=jnp.float32).astype(jnp.bfloat16).reshape(length, HEADS, DV)
        stacked = jnp.concatenate([query, key_rows, value_rows], axis=2)
        normed = mechanism(stacked, log_decay).reshape(length, HEADS * DV)
        return jnp.dot(normed, output_weight, preferred_element_type=jnp.float32).astype(jnp.bfloat16)
    return lax.map(one_sequence, tokens)
```

```python
import functools

import numpy as np
import jax
import jax.numpy as jnp
from jax import lax
from jax.experimental import pallas as pl
from jax.experimental.pallas import tpu as pltpu
from jax.sharding import PartitionSpec as P

HEADS = 16
DK = 64
DV = 128
BLOCK = 512


exact_precision = lax.Precision.HIGHEST


def rotate(values_part, positions):
    half_dim = values_part.shape[-1] // 2
    frequency = 10000.0 ** (-jnp.arange(half_dim, dtype=jnp.float32) / half_dim)
    angles = positions[:, None] * frequency[None, :]
    cosine = jnp.cos(angles)[:, None, :]
    sine_part = jnp.sin(angles)[:, None, :]
    first = values_part[..., :half_dim]
    second = values_part[..., half_dim:]
    return jnp.concatenate(
        [first * cosine - second * sine_part, first * sine_part + second * cosine], axis=-1
    )


def retain(query, key_rows, value_rows, log_rate):
    length, heads, key_dim = query.shape
    value_dim = value_rows.shape[-1]
    count = length // BLOCK
    offsets = jnp.arange(BLOCK, dtype=jnp.float32)
    distance = offsets[:, None] - offsets[None, :]
    decay_inner = jnp.where(
        distance[None] >= 0.0,
        jnp.exp(log_rate[:, None, None] * jnp.maximum(distance, 0.0)[None]),
        0.0,
    )
    decay_query = jnp.exp((offsets[:, None] + 1.0) * log_rate[None, :])[:, :, None]
    decay_key = jnp.exp((BLOCK - 1.0 - offsets)[:, None] * log_rate[None, :])[:, :, None]
    decay_block = jnp.exp(BLOCK * log_rate)[:, None, None]

    def blocks(array):
        return array.reshape(count, BLOCK, heads, array.shape[-1])

    def advance(state, inputs):
        query_block, key_block, value_block = inputs
        inner = (
            jnp.einsum("ihd,jhd->hij", query_block, key_block, preferred_element_type=jnp.float32)
            * decay_inner
        )
        result = jnp.einsum(
            "hij,jhv->ihv",
            inner.astype(jnp.bfloat16),
            value_block,
            preferred_element_type=jnp.float32,
        )
        query_wide = query_block.astype(jnp.float32) * decay_query
        result = result + jnp.einsum("ihd,hdv->ihv", query_wide, state, precision=exact_precision)
        key_wide = key_block.astype(jnp.float32) * decay_key
        state = state * decay_block + jnp.einsum(
            "jhd,jhv->hdv", key_wide, value_block.astype(jnp.float32), precision=exact_precision
        )
        return (state, result)

    initial = jnp.zeros((heads, key_dim, value_dim), jnp.float32)
    final_state, outputs = lax.scan(
        advance, initial, (blocks(query), blocks(key_rows), blocks(value_rows))
    )
    return outputs.reshape(length, heads, value_dim)


def mechanism(stacked, log_decay):
    length = stacked.shape[0]
    widened = stacked[..., : 2 * DK].astype(jnp.float32)
    positions = jnp.arange(length, dtype=jnp.float32)
    query = rotate(widened[..., :DK], positions).astype(jnp.bfloat16)
    key_rows = rotate(widened[..., DK : 2 * DK], positions).astype(jnp.bfloat16)
    value_rows = stacked[..., 2 * DK :]
    forward = retain(query, key_rows, value_rows, log_decay[0])
    backward = retain(
        jnp.flip(query, 0), jnp.flip(key_rows, 0), jnp.flip(value_rows, 0), log_decay[1]
    )
    combined = forward + jnp.flip(backward, 0)
    average = jnp.mean(combined, axis=-1, keepdims=True)
    centred = combined - average
    variance = jnp.mean(centred * centred, axis=-1, keepdims=True)
    return (centred * lax.rsqrt(variance + 1e-06)).astype(jnp.bfloat16)


def shards(tokens, query_weight, key_weight, value_weight, output_weight, log_decay):
    rows = tokens[0]
    row_count = rows.shape[0]
    local_heads = log_decay.shape[1]
    first_head = lax.axis_index("sp") * local_heads
    own_slices = jnp.concatenate(
        [
            lax.dynamic_slice_in_dim(query_weight, first_head * DK, local_heads * DK, 1),
            lax.dynamic_slice_in_dim(key_weight, first_head * DK, local_heads * DK, 1),
            lax.dynamic_slice_in_dim(value_weight, first_head * DV, local_heads * DV, 1),
        ],
        axis=1,
    )
    own_whole = lax.all_gather(own_slices, "dp", axis=0, tiled=True)
    piece = lax.all_gather(rows, "sp", axis=0, tiled=True)
    count = piece.shape[0]
    product = jnp.dot(piece, own_whole, preferred_element_type=jnp.float32).astype(jnp.bfloat16)
    query_part = product[:, : local_heads * DK].reshape(count, local_heads, DK)
    key_part = product[:, local_heads * DK : 2 * local_heads * DK].reshape(count, local_heads, DK)
    value_part = product[:, 2 * local_heads * DK :].reshape(count, local_heads, DV)
    gathered = jnp.concatenate([query_part, key_part, value_part], axis=2)
    normed = mechanism(gathered, log_decay)
    by_token = lax.all_to_all(normed, "sp", split_axis=0, concat_axis=1, tiled=True).reshape(
        row_count, HEADS * DV
    )
    mixed = jnp.dot(
        by_token,
        lax.all_gather(output_weight, "dp", axis=0, tiled=True),
        preferred_element_type=jnp.float32,
    )
    return mixed.astype(jnp.bfloat16)[None]


MESH = pl.DeviceIdType.MESH
CORES = 2
PAIR = 2
PIECES = 2
LANES = PAIR * DK


def tables(length):
    half = DK // 2
    frequency = (10000.0 ** (-np.arange(half) / half)).astype(np.float32)
    angles = (np.arange(length, dtype=np.float32)[:, None] * frequency[None, :]).astype(np.float64)
    cosine = np.tile(np.cos(angles), (1, 4)).astype(np.float32)
    sine = np.tile(np.sin(angles), (1, 4)).astype(np.float32)
    swap = np.zeros((LANES, LANES), np.float32)
    for lane in range(LANES):
        if lane % DK < half:
            swap[lane + half, lane] = -1.0
        else:
            swap[lane - half, lane] = 1.0
    return jnp.asarray(cosine), jnp.asarray(sine), jnp.asarray(swap, jnp.bfloat16)


def layer_kernel(
    S, Z, rate_hbm, cos_hbm, sin_hbm, swap_hbm, x_ref, wq_ref, wk_ref, wv_ref, wo_ref, out_ref,
    tok, wqkv, wo, acc, decay, qk, val, sc, nown, nrm, oacc, cos_ref, sin_ref, swap_ref, rate_ref,
    lsem, send, tR, rR, qR, qpR, oR, iR, jR, dR, opR, nR,
):
    s = lax.axis_index("sp")
    d = lax.axis_index("dp")
    z, c = d // CORES, d % CORES
    rows, model = x_ref.shape
    length = S * rows
    depth = wq_ref.shape[0]
    heads = rate_hbm.shape[1]
    groups = heads // PAIR
    qc, vc = heads * DK, heads * DV
    wide_v = PAIR * DV
    width = 2 * LANES + wide_v
    oc = wo.shape[3]
    step_rows = depth // PIECES
    half_model = model // 2
    sx = s + 1 - 2 * (s % 2)
    sy = (s + 2) % 4
    sd = (sx + 2) % 4
    partner = {"dp": z * CORES + 1 - c}
    end = (z == 0) | (z == Z - 1)
    mid = jnp.logical_not(end)

    near, across, mirror = z + 1 - 2 * (z % 2), (z + 2) % Z, Z - 1 - z
    second = jnp.where(end, across, mirror)
    third = jnp.where(end, mirror, across)
    o_first = jnp.where(end, near, mirror)
    o_second = jnp.where(end, across, near)

    def remote(src, send_at, recv, device, dst=None):
        return pltpu.make_async_remote_copy(
            src_ref=src, dst_ref=src if dst is None else dst, send_sem=send.at[send_at], recv_sem=recv,
            device_id=device, device_id_type=MESH,
        )

    def local(src, dst, at):
        return pltpu.make_async_copy(src, dst, lsem.at[at])

    def weight_copies(group):
        def part(ref, at, size, to):
            cols = pl.ds(pl.multiple_of(at + group * size, size), size)
            return local(ref.at[:, cols], wqkv.at[d, group, :, pl.ds(to, size)], group)

        return [
            part(wq_ref, s * qc, LANES, 0), part(wk_ref, s * qc, LANES, LANES),
            part(wv_ref, s * vc, wide_v, 2 * LANES),
        ]

    def quarter_copy(j):
        at = (s + j) % S
        return local(wo_ref.at[:, pl.ds(pl.multiple_of(at * oc, oc), oc)], wo.at[d, at], 3 if j == 0 else 4)

    def local_wait(ref, at):
        local(ref, ref, at).wait()

    local_c = [
        local(rate_hbm, rate_ref, 5), local(cos_hbm, cos_ref, 6),
        local(sin_hbm, sin_ref, 7), local(swap_hbm, swap_ref, 8),
    ]
    for copy in (
        weight_copies(0) + [local(x_ref, tok.at[s], 2), quarter_copy(0)] + weight_copies(1)
        + local_c[:1] + [quarter_copy(j) for j in range(1, S)] + local_c[1:]
    ):
        copy.start()

    barrier = pltpu.get_barrier_semaphore()

    def greet(device):
        pl.semaphore_signal(barrier, inc=1, device_id=device, device_id_type=MESH)

    pl.when(z > 0)(lambda: greet({"dp": d - CORES}))
    pl.when(z < Z - 1)(lambda: greet({"dp": d + CORES}))
    for other in range(1, S):
        greet({"sp": (s + other) % S})
    greet(partner)
    pl.when(mid)(lambda: pl.semaphore_wait(barrier, S + 2))
    pl.when(end)(lambda: pl.semaphore_wait(barrier, S + 1))

    def side(way):
        return {"dp": d + CORES - 2 * CORES * way}

    def way_of(src):
        return jnp.where(src < z, 0, 1)

    def q_ref(block, item):
        if item == 0:
            return wqkv.at[block, 0]
        return wqkv.at[block, 1, :, pl.ds((item - 1) * 2 * LANES, 2 * LANES)]

    def q_copy(way, src, item):
        return remote(q_ref(src * CORES + c, item), 0, qR.at[src, item], side(way))

    def qp_copy(src, item, mine=True):
        return remote(q_ref(src * CORES + (c if mine else 1 - c), item), 2, qpR.at[src, item], partner)

    def o_piece(block, quarter, piece):
        return wo.at[block, quarter, pl.ds(piece * step_rows, step_rows)]

    def o_copy(way, src, piece):
        return remote(o_piece(src * CORES + c, s, piece), 1, oR.at[src, piece], side(way))

    def op_copy(src, quarter):
        return remote(wo.at[src * CORES + c, quarter], 3, opR.at[src], partner)

    def i_copy(axis, src, piece, mine=True):
        to = sx if axis == 0 else sy
        recv = iR.at[axis, src] if axis == piece else jR.at[src]
        return remote(o_piece(src * CORES + c, s if mine else to, piece), 4, recv, {"sp": to})

    def d_copy(src, piece):
        to, quarter = (sy, sx) if piece == 0 else (sx, sy)
        return remote(o_piece(src * CORES + c, quarter, piece), 5, dR.at[src], {"sp": to})

    def t_ref(block, half):
        return tok.at[block, :, pl.ds(half * half_model, half_model)]

    def t_copy(axis, half, mine=True):
        to = sx if axis == 0 else sy
        return remote(t_ref(s if mine else to, half), 6, tR.at[axis, half], {"sp": to})

    def r_copy(half, mine=True):
        to, block = (sy, sx) if half == 0 else (sx, sy)
        return remote(t_ref(block if mine else sd, half), 6, rR.at[half], {"sp": to})

    def n_copy(head, to):
        return remote(
            nown.at[head, pl.ds(pl.multiple_of(to * rows, rows), rows)], 7, nR.at[head // PAIR, s], {"sp": to},
            dst=nrm.at[s, :, pl.ds(head * DV, DV)],
        )

    def n_wait(group, j):
        ref = nrm.at[j, :, pl.ds(group * wide_v, wide_v)]
        remote(ref, 7, nR.at[group, j], {"sp": j}).wait_recv()

    def ways(fn):
        for way in (0, 1):
            pl.when(z < Z - 1 if way == 0 else z > 0)(functools.partial(fn, way))

    def start_all(copies):
        for copy in copies:
            copy.start()

    def own_q(items):
        ways(lambda way: start_all([q_copy(way, z, item) for item in items]))

    def own_o():
        ways(lambda way: start_all([o_copy(way, z, piece) for piece in range(PIECES)]))

    local_wait(wqkv.at[d, 0], 0)
    own_q((0,))
    local_wait(tok.at[s], 2)
    for half in range(2):
        t_copy(0, half).start()
        t_copy(1, 1 - half).start()
    qp_copy(z, 0).start()
    local_wait(wo.at[d, s], 3)
    own_o()
    local_wait(wqkv.at[d, 1], 1)
    pl.when(end)(lambda: own_q((1, 2)))
    qp_copy(z, 1).start()
    qp_copy(z, 2).start()

    def decays(group):
        for head in range(group * PAIR, (group + 1) * PAIR):
            fast, slow = rate_ref[0, head], rate_ref[1, head]

            @pl.loop(0, S)
            def _(j):
                at = lax.broadcasted_iota(jnp.int32, (rows, length), 0) + j * rows
                gap = (at - lax.broadcasted_iota(jnp.int32, (rows, length), 1)).astype(jnp.float32)
                weight = jnp.exp(jnp.where(gap >= 0.0, gap * fast, gap * (-slow)))
                decay[head, pl.ds(pl.multiple_of(j * rows, rows), rows), :] = jnp.where(gap == 0.0, 2.0, weight)

    def q_step(src, items):
        way = way_of(src)
        onward = jnp.where(src < z, z < Z - 1, z > 0)
        for item in items:
            q_copy(1 - way, src, item).wait_recv()
            pl.when(onward)(lambda: q_copy(way, src, item).start())
            qp_copy(src, item).start()

    def o_step(src):
        way = way_of(src)
        onward = jnp.where(src < z, z < Z - 1, z > 0)
        for piece in range(PIECES):
            o_copy(1 - way, src, piece).wait_recv()
            pl.when(onward)(lambda: o_copy(way, src, piece).start())
            i_copy(piece, src, piece).start()
            i_copy(1 - piece, src, piece).start()
        op_copy(src, s).start()

    def o_relay(src):
        for piece in range(PIECES):
            i_copy(piece, src, piece, mine=False).wait_recv()
            d_copy(src, piece).start()

    def o_share(src):
        remote(wo.at[src * CORES + c, sx], 4, jR.at[src], {"sp": sx}).wait_recv()
        op_copy(src, sx).start()
        op_copy(src, sy).start()
        remote(wo.at[src * CORES + c, sd], 5, dR.at[src], {"sp": sx}).wait_recv()
        op_copy(src, sd).start()

    def o_ready(src):
        remote(wo.at[src * CORES + 1 - c], 3, opR.at[src], partner).wait_recv()

    tile = 2 * LANES

    def project(src, group, parts, first=False):
        wide = CORES * depth
        cols = pl.ds(pl.multiple_of(src * wide, wide), wide)
        for n in parts:
            at = slice(n * tile, (n + 1) * tile)
            part = jnp.dot(
                tok[:, :, cols].reshape(length, wide),
                wqkv[pl.ds(src * CORES, CORES), group, :, at].reshape(wide, tile),
                preferred_element_type=jnp.float32,
            )
            if first:
                acc[group, :, at] = part
            else:
                acc[group, :, at] += part

    def project_a(src, first=False):
        qp_copy(src, 0, mine=False).wait_recv()
        project(src, 0, (0, 1), first)

    def project_b(src, first=False, parts=(0, 1)):
        for n in parts:
            qp_copy(src, 1 + n, mine=False).wait_recv()
        project(src, 1, parts, first)

    def scores(group):
        for part in range(2):
            at = slice(part * LANES, (part + 1) * LANES)
            flat = acc[group, :, at].astype(jnp.bfloat16)
            turned = jnp.dot(flat, swap_ref[...], preferred_element_type=jnp.float32)
            qk[group, :, at] = (flat.astype(jnp.float32) * cos_ref[...] + turned * sin_ref[...]).astype(jnp.bfloat16)
        lane = lax.broadcasted_iota(jnp.int32, (length, LANES), 1)
        for inner in range(PAIR):
            query = qk[group, :, :LANES]
            query = jnp.where((lane // DK) == inner, query.astype(jnp.float32), 0.0).astype(jnp.bfloat16)
            for n in range(length // tile):
                at = slice(n * tile, (n + 1) * tile)
                part = lax.dot_general(
                    query, qk[group, at, LANES:], (((1,), (1,)), ((), ())), preferred_element_type=jnp.float32,
                )
                sc[inner, :, at] = (part * decay[group * PAIR + inner, :, at]).astype(jnp.bfloat16)

    def values(group):
        val[group] = acc[group, :, 2 * LANES :].astype(jnp.bfloat16)
        for inner in range(PAIR):
            head = group * PAIR + inner
            ret = jnp.dot(sc[inner], val[group, :, inner * DV : (inner + 1) * DV], preferred_element_type=jnp.float32)
            centred = ret - jnp.mean(ret, axis=-1, keepdims=True)
            variance = jnp.mean(centred * centred, axis=-1, keepdims=True)
            nown[head] = (centred * lax.rsqrt(variance + 1e-06)).astype(jnp.bfloat16)
            for to in (sd, sx, sy):
                n_copy(head, to).start()
            nrm[s, :, head * DV : (head + 1) * DV] = nown[head, pl.ds(pl.multiple_of(s * rows, rows), rows), :]

    def finish(units, first=False, last=False):
        for src, group in units:
            pl.when(src != s)(lambda: n_wait(group, src))
        for j in range(S):
            at = slice(j * oc, (j + 1) * oc)
            total = None if first else oacc[:, at]
            for src, group in units:
                part = jnp.dot(
                    nrm[src, :, group * wide_v : (group + 1) * wide_v], wo[src * CORES + group, j],
                    preferred_element_type=jnp.float32,
                )
                total = part if total is None else total + part
            if last:
                out_ref[:, at] = total.astype(out_ref.dtype)
            else:
                oacc[:, at] = total

    def on(where, fn, *args):
        pl.when(where)(lambda: fn(*args))

    both = (1, 2)
    local_wait(wo.at[pl.ds(0, S - 1), 0], 4)
    for j in range(S):
        op_copy(z, (s + j) % S).start()
    local_c[0].wait()
    decays(0)
    for half in range(2):
        t_copy(half, half, mine=False).wait_recv()
        r_copy(half).start()
    q_step(near, (0,))
    on(mid, q_step, second, (0,))
    o_step(o_first)
    on(mid, own_q, both)
    on(mid, q_step, near, both)
    for copy in local_c[1:]:
        copy.wait()
    t_copy(0, 1, mine=False).wait_recv()
    t_copy(1, 0, mine=False).wait_recv()
    for half in range(2):
        r_copy(half, mine=False).wait_recv()
    project_a(z, True)
    project_a(near)
    on(end, q_step, second, (0,))
    project_a(second)
    o_step(o_second)
    o_relay(o_first)
    on(end, q_step, near, both)
    q_step(third, (0,))
    on(mid, q_step, second, both)
    project_a(third)
    scores(0)
    values(0)
    decays(1)
    o_share(o_first)
    o_relay(o_second)
    on(mid, o_step, third)
    project_b(z, True)
    project_b(near)
    on(end, q_step, second, both)
    project_b(second)
    o_ready(z)
    o_ready(o_first)
    finish(((z, 0), (o_first, 0)), first=True)
    o_share(o_second)
    on(end, o_step, third)
    o_ready(o_second)
    finish(((o_second, 0),))
    o_relay(third)
    q_step(third, (1,))
    project_b(third, parts=(0,))
    scores(1)
    q_step(third, (2,))
    project_b(third, parts=(1,))
    values(1)
    o_share(third)
    finish(((z, 1), (o_first, 1), (o_second, 1)))
    o_ready(third)
    finish(((third, 0), (third, 1)), last=True)

    def sent(ref, at):
        remote(ref, at, tR.at[0, 0], partner).wait_send()

    for where, count in ((mid, Z + 1), (end, 1)):
        @pl.when(where)
        def _():
            sent(wqkv.at[pl.ds(0, count)], 0)
            sent(wo.at[pl.ds(0, count), 0], 1)
    sent(wqkv.at[pl.ds(0, Z)], 2)
    sent(wo.at[pl.ds(0, Z)], 3)
    sent(wo.at[pl.ds(0, Z - 1), pl.ds(0, 2)], 4)
    sent(wo.at[pl.ds(0, Z - 1), 0], 5)
    sent(tok.at[pl.ds(0, S - 1)], 6)
    sent(nown.at[:, pl.ds(0, (S - 1) * rows)], 7)


def fused(S, Z, tokens, query_weight, key_weight, value_weight, output_weight, log_decay):
    rows, model = tokens.shape[1:]
    depth = query_weight.shape[0]
    heads = log_decay.shape[1]
    groups = heads // PAIR
    length = S * rows
    width = 2 * LANES + PAIR * DV
    oc = output_weight.shape[1] // S
    cosine, sine, swap = tables(length)
    anyplace = pl.BlockSpec(memory_space=pl.ANY)
    dma = pltpu.SemaphoreType.DMA
    bf, f32 = jnp.bfloat16, jnp.float32
    out = pl.pallas_call(
        functools.partial(layer_kernel, S, Z),
        out_shape=pltpu.VMEM((rows, output_weight.shape[1]), bf),
        in_specs=[anyplace] * 9,
        out_specs=pl.BlockSpec(memory_space=pltpu.VMEM),
        scratch_shapes=[
            pltpu.VMEM((S, rows, model), bf),
            pltpu.VMEM((Z * CORES, groups, depth, width), bf),
            pltpu.VMEM((Z * CORES, S, depth, oc), bf),
            pltpu.VMEM((groups, length, width), f32),
            pltpu.VMEM((heads, length, length), f32),
            pltpu.VMEM((groups, length, 2 * LANES), bf),
            pltpu.VMEM((groups, length, PAIR * DV), bf),
            pltpu.VMEM((PAIR, length, length), bf),
            pltpu.VMEM((heads, length, DV), bf),
            pltpu.VMEM((S, rows, heads * DV), bf),
            pltpu.VMEM((rows, S * oc), f32),
            pltpu.VMEM((length, LANES), f32), pltpu.VMEM((length, LANES), f32), pltpu.VMEM((LANES, LANES), bf),
            pltpu.SMEM((2, heads), f32),
            dma((9,)), dma((8,)), dma((2, 2)), dma((2,)), dma((Z, 3)), dma((Z, 3)),
            dma((Z, PIECES)), dma((2, Z)), dma((Z,)), dma((Z,)), dma((Z,)), dma((groups, S)),
        ],
        compiler_params=pltpu.CompilerParams(
            collective_id=0, has_side_effects=True, vmem_limit_bytes=56 * 1024 * 1024
        ),
    )(log_decay, cosine, sine, swap, tokens[0], query_weight, key_weight, value_weight, output_weight)
    return out[None]


def solution(mesh):
    S, D = mesh.shape["sp"], mesh.shape["dp"]
    Z = D // CORES

    def layer(tokens, query_weight, key_weight, value_weight, output_weight, log_decay):
        rows = tokens.shape[1]
        depth = query_weight.shape[0]
        heads = log_decay.shape[1]
        fits = (
            S == 4 and Z == 4 and D == CORES * Z and S * rows == BLOCK and heads == CORES * PAIR
            and PAIR * DV == depth and rows % 128 == 0
        )
        args = (tokens, query_weight, key_weight, value_weight, output_weight, log_decay)
        return fused(S, Z, *args) if fits else shards(*args)

    placed = (
        P("dp", "sp", None),
        P("dp", None),
        P("dp", None),
        P("dp", None),
        P("dp", None),
        P(None, "sp"),
    )
    return jax.shard_map(
        layer, mesh=mesh, in_specs=placed, out_specs=P("dp", "sp", None), check_vma=False
    )
```

```python
import functools

import numpy as np
import jax
import jax.numpy as jnp
from jax import lax
from jax.experimental import pallas as pl
from jax.experimental.pallas import tpu as pltpu
from jax.sharding import PartitionSpec as P

HEADS = 16
DK = 64
DV = 128
BLOCK = 512


exact_precision = lax.Precision.HIGHEST


def rotate(values_part, positions):
    half_dim = values_part.shape[-1] // 2
    frequency = 10000.0 ** (-jnp.arange(half_dim, dtype=jnp.float32) / half_dim)
    angles = positions[:, None] * frequency[None, :]
    cosine = jnp.cos(angles)[:, None, :]
    sine_part = jnp.sin(angles)[:, None, :]
    first = values_part[..., :half_dim]
    second = values_part[..., half_dim:]
    return jnp.concatenate(
        [first * cosine - second * sine_part, first * sine_part + second * cosine], axis=-1
    )


def retain(query, key_rows, value_rows, log_rate):
    length, heads, key_dim = query.shape
    value_dim = value_rows.shape[-1]
    count = length // BLOCK
    offsets = jnp.arange(BLOCK, dtype=jnp.float32)
    distance = offsets[:, None] - offsets[None, :]
    decay_inner = jnp.where(
        distance[None] >= 0.0,
        jnp.exp(log_rate[:, None, None] * jnp.maximum(distance, 0.0)[None]),
        0.0,
    )
    decay_query = jnp.exp((offsets[:, None] + 1.0) * log_rate[None, :])[:, :, None]
    decay_key = jnp.exp((BLOCK - 1.0 - offsets)[:, None] * log_rate[None, :])[:, :, None]
    decay_block = jnp.exp(BLOCK * log_rate)[:, None, None]

    def blocks(array):
        return array.reshape(count, BLOCK, heads, array.shape[-1])

    def advance(state, inputs):
        query_block, key_block, value_block = inputs
        inner = (
            jnp.einsum("ihd,jhd->hij", query_block, key_block, preferred_element_type=jnp.float32)
            * decay_inner
        )
        result = jnp.einsum(
            "hij,jhv->ihv",
            inner.astype(jnp.bfloat16),
            value_block,
            preferred_element_type=jnp.float32,
        )
        query_wide = query_block.astype(jnp.float32) * decay_query
        result = result + jnp.einsum("ihd,hdv->ihv", query_wide, state, precision=exact_precision)
        key_wide = key_block.astype(jnp.float32) * decay_key
        state = state * decay_block + jnp.einsum(
            "jhd,jhv->hdv", key_wide, value_block.astype(jnp.float32), precision=exact_precision
        )
        return (state, result)

    initial = jnp.zeros((heads, key_dim, value_dim), jnp.float32)
    final_state, outputs = lax.scan(
        advance, initial, (blocks(query), blocks(key_rows), blocks(value_rows))
    )
    return outputs.reshape(length, heads, value_dim)


def mechanism(stacked, log_decay):
    length = stacked.shape[0]
    widened = stacked[..., : 2 * DK].astype(jnp.float32)
    positions = jnp.arange(length, dtype=jnp.float32)
    query = rotate(widened[..., :DK], positions).astype(jnp.bfloat16)
    key_rows = rotate(widened[..., DK : 2 * DK], positions).astype(jnp.bfloat16)
    value_rows = stacked[..., 2 * DK :]
    forward = retain(query, key_rows, value_rows, log_decay[0])
    backward = retain(
        jnp.flip(query, 0), jnp.flip(key_rows, 0), jnp.flip(value_rows, 0), log_decay[1]
    )
    combined = forward + jnp.flip(backward, 0)
    average = jnp.mean(combined, axis=-1, keepdims=True)
    centred = combined - average
    variance = jnp.mean(centred * centred, axis=-1, keepdims=True)
    return (centred * lax.rsqrt(variance + 1e-06)).astype(jnp.bfloat16)


def shards(tokens, query_weight, key_weight, value_weight, output_weight, log_decay):
    rows = tokens[0]
    row_count = rows.shape[0]
    local_heads = log_decay.shape[1]
    first_head = lax.axis_index("sp") * local_heads
    own_slices = jnp.concatenate(
        [
            lax.dynamic_slice_in_dim(query_weight, first_head * DK, local_heads * DK, 1),
            lax.dynamic_slice_in_dim(key_weight, first_head * DK, local_heads * DK, 1),
            lax.dynamic_slice_in_dim(value_weight, first_head * DV, local_heads * DV, 1),
        ],
        axis=1,
    )
    own_whole = lax.all_gather(own_slices, "dp", axis=0, tiled=True)
    piece = lax.all_gather(rows, "sp", axis=0, tiled=True)
    count = piece.shape[0]
    product = jnp.dot(piece, own_whole, preferred_element_type=jnp.float32).astype(jnp.bfloat16)
    query_part = product[:, : local_heads * DK].reshape(count, local_heads, DK)
    key_part = product[:, local_heads * DK : 2 * local_heads * DK].reshape(count, local_heads, DK)
    value_part = product[:, 2 * local_heads * DK :].reshape(count, local_heads, DV)
    gathered = jnp.concatenate([query_part, key_part, value_part], axis=2)
    normed = mechanism(gathered, log_decay)
    by_token = lax.all_to_all(normed, "sp", split_axis=0, concat_axis=1, tiled=True).reshape(
        row_count, HEADS * DV
    )
    mixed = jnp.dot(
        by_token,
        lax.all_gather(output_weight, "dp", axis=0, tiled=True),
        preferred_element_type=jnp.float32,
    )
    return mixed.astype(jnp.bfloat16)[None]


MESH = pl.DeviceIdType.MESH
CORES = 2
PAIR = 2
PIECES = 2
LANES = PAIR * DK


def tables(length):
    half = DK // 2
    frequency = (10000.0 ** (-np.arange(half) / half)).astype(np.float32)
    angles = (np.arange(length, dtype=np.float32)[:, None] * frequency[None, :]).astype(np.float64)
    cosine = np.tile(np.cos(angles), (1, 4)).astype(np.float32)
    sine = np.tile(np.sin(angles), (1, 4)).astype(np.float32)
    swap = np.zeros((LANES, LANES), np.float32)
    for lane in range(LANES):
        if lane % DK < half:
            swap[lane + half, lane] = -1.0
        else:
            swap[lane - half, lane] = 1.0
    return jnp.asarray(cosine), jnp.asarray(sine), jnp.asarray(swap, jnp.bfloat16)


def layer_kernel(
    S, Z, rate_hbm, cos_hbm, sin_hbm, swap_hbm, x_ref, wq_ref, wk_ref, wv_ref, wo_ref, out_ref,
    tok, wqkv, wo, acc, decay, qk, val, sc, nown, nrm, oacc, cos_ref, sin_ref, swap_ref, rate_ref,
    lsem, send, tR, rR, qR, qpR, oR, iR, jR, dR, opR, nR,
):
    s = lax.axis_index("sp")
    d = lax.axis_index("dp")
    z, c = d // CORES, d % CORES
    rows, model = x_ref.shape
    length = S * rows
    depth = wq_ref.shape[0]
    heads = rate_hbm.shape[1]
    groups = heads // PAIR
    qc, vc = heads * DK, heads * DV
    wide_v = PAIR * DV
    width = 2 * LANES + wide_v
    oc = wo.shape[3]
    step_rows = depth // PIECES
    half_model = model // 2
    sx = s + 1 - 2 * (s % 2)
    sy = (s + 2) % 4
    sd = (sx + 2) % 4
    partner = {"dp": z * CORES + 1 - c}
    end = (z == 0) | (z == Z - 1)
    mid = jnp.logical_not(end)

    near, across, mirror = z + 1 - 2 * (z % 2), (z + 2) % Z, Z - 1 - z
    second = jnp.where(end, across, mirror)
    third = jnp.where(end, mirror, across)
    o_first = jnp.where(end, near, mirror)
    o_second = jnp.where(end, across, near)

    def remote(src, send_at, recv, device, dst=None):
        return pltpu.make_async_remote_copy(
            src_ref=src, dst_ref=src if dst is None else dst, send_sem=send.at[send_at], recv_sem=recv,
            device_id=device, device_id_type=MESH,
        )

    def local(src, dst, at):
        return pltpu.make_async_copy(src, dst, lsem.at[at])

    def weight_copies(group):
        def part(ref, at, size, to):
            cols = pl.ds(pl.multiple_of(at + group * size, size), size)
            return local(ref.at[:, cols], wqkv.at[d, group, :, pl.ds(to, size)], group)

        return [
            part(wq_ref, s * qc, LANES, 0), part(wk_ref, s * qc, LANES, LANES),
            part(wv_ref, s * vc, wide_v, 2 * LANES),
        ]

    def quarter_copy(j):
        at = (s + j) % S
        return local(wo_ref.at[:, pl.ds(pl.multiple_of(at * oc, oc), oc)], wo.at[d, at], 3 if j == 0 else 4)

    def local_wait(ref, at):
        local(ref, ref, at).wait()

    local_c = [
        local(rate_hbm, rate_ref, 5), local(cos_hbm, cos_ref, 6),
        local(sin_hbm, sin_ref, 7), local(swap_hbm, swap_ref, 8),
    ]
    for copy in (
        weight_copies(0) + [local(x_ref, tok.at[s], 2), quarter_copy(0)] + weight_copies(1)
        + local_c[:1] + [quarter_copy(j) for j in range(1, S)] + local_c[1:]
    ):
        copy.start()

    barrier = pltpu.get_barrier_semaphore()

    def greet(device):
        pl.semaphore_signal(barrier, inc=1, device_id=device, device_id_type=MESH)

    pl.when(z > 0)(lambda: greet({"dp": d - CORES}))
    pl.when(z < Z - 1)(lambda: greet({"dp": d + CORES}))
    for other in range(1, S):
        greet({"sp": (s + other) % S})
    greet(partner)
    pl.when(mid)(lambda: pl.semaphore_wait(barrier, S + 2))
    pl.when(end)(lambda: pl.semaphore_wait(barrier, S + 1))

    def side(way):
        return {"dp": d + CORES - 2 * CORES * way}

    def way_of(src):
        return jnp.where(src < z, 0, 1)

    def q_ref(block, item):
        if item == 0:
            return wqkv.at[block, 0]
        return wqkv.at[block, 1, :, pl.ds((item - 1) * 2 * LANES, 2 * LANES)]

    def q_copy(way, src, item):
        return remote(q_ref(src * CORES + c, item), 0, qR.at[src, item], side(way))

    def qp_copy(src, item, mine=True):
        return remote(q_ref(src * CORES + (c if mine else 1 - c), item), 2, qpR.at[src, item], partner)

    def o_piece(block, quarter, piece):
        return wo.at[block, quarter, pl.ds(piece * step_rows, step_rows)]

    def o_copy(way, src, piece):
        return remote(o_piece(src * CORES + c, s, piece), 1, oR.at[src, piece], side(way))

    def op_copy(src, quarter):
        return remote(wo.at[src * CORES + c, quarter], 3, opR.at[src], partner)

    def i_copy(axis, src, piece, mine=True):
        to = sx if axis == 0 else sy
        recv = iR.at[axis, src] if axis == piece else jR.at[src]
        return remote(o_piece(src * CORES + c, s if mine else to, piece), 4, recv, {"sp": to})

    def d_copy(src, piece):
        to, quarter = (sy, sx) if piece == 0 else (sx, sy)
        return remote(o_piece(src * CORES + c, quarter, piece), 5, dR.at[src], {"sp": to})

    def t_ref(block, half):
        return tok.at[block, :, pl.ds(half * half_model, half_model)]

    def t_copy(axis, half, mine=True):
        to = sx if axis == 0 else sy
        return remote(t_ref(s if mine else to, half), 6, tR.at[axis, half], {"sp": to})

    def r_copy(half, mine=True):
        to, block = (sy, sx) if half == 0 else (sx, sy)
        return remote(t_ref(block if mine else sd, half), 6, rR.at[half], {"sp": to})

    def n_copy(head, to):
        return remote(
            nown.at[head, pl.ds(pl.multiple_of(to * rows, rows), rows)], 7, nR.at[head // PAIR, s], {"sp": to},
            dst=nrm.at[s, :, pl.ds(head * DV, DV)],
        )

    def n_wait(group, j):
        ref = nrm.at[j, :, pl.ds(group * wide_v, wide_v)]
        remote(ref, 7, nR.at[group, j], {"sp": j}).wait_recv()

    def ways(fn):
        for way in (0, 1):
            pl.when(z < Z - 1 if way == 0 else z > 0)(functools.partial(fn, way))

    def start_all(copies):
        for copy in copies:
            copy.start()

    def own_q(items):
        ways(lambda way: start_all([q_copy(way, z, item) for item in items]))

    def own_o():
        ways(lambda way: start_all([o_copy(way, z, piece) for piece in range(PIECES)]))

    local_wait(wqkv.at[d, 0], 0)
    own_q((0,))
    local_wait(tok.at[s], 2)
    for half in range(2):
        t_copy(0, half).start()
        t_copy(1, 1 - half).start()
    qp_copy(z, 0).start()
    local_wait(wo.at[d, s], 3)
    own_o()
    local_wait(wqkv.at[d, 1], 1)
    pl.when(end)(lambda: own_q((1, 2)))
    qp_copy(z, 1).start()
    qp_copy(z, 2).start()

    def decays(group):
        for head in range(group * PAIR, (group + 1) * PAIR):
            fast, slow = rate_ref[0, head], rate_ref[1, head]

            @pl.loop(0, S)
            def _(j):
                at = lax.broadcasted_iota(jnp.int32, (rows, length), 0) + j * rows
                gap = (at - lax.broadcasted_iota(jnp.int32, (rows, length), 1)).astype(jnp.float32)
                weight = jnp.exp(jnp.where(gap >= 0.0, gap * fast, gap * (-slow)))
                decay[head, pl.ds(pl.multiple_of(j * rows, rows), rows), :] = jnp.where(gap == 0.0, 2.0, weight)

    def q_step(src, items):
        way = way_of(src)
        onward = jnp.where(src < z, z < Z - 1, z > 0)
        for item in items:
            q_copy(1 - way, src, item).wait_recv()
            pl.when(onward)(lambda: q_copy(way, src, item).start())
            qp_copy(src, item).start()

    def o_step(src):
        way = way_of(src)
        onward = jnp.where(src < z, z < Z - 1, z > 0)
        for piece in range(PIECES):
            o_copy(1 - way, src, piece).wait_recv()
            pl.when(onward)(lambda: o_copy(way, src, piece).start())
            i_copy(piece, src, piece).start()
            i_copy(1 - piece, src, piece).start()
        op_copy(src, s).start()

    def o_relay(src):
        for piece in range(PIECES):
            i_copy(piece, src, piece, mine=False).wait_recv()
            d_copy(src, piece).start()

    def o_share(src):
        remote(wo.at[src * CORES + c, sx], 4, jR.at[src], {"sp": sx}).wait_recv()
        op_copy(src, sx).start()
        op_copy(src, sy).start()
        remote(wo.at[src * CORES + c, sd], 5, dR.at[src], {"sp": sx}).wait_recv()
        op_copy(src, sd).start()

    def o_ready(src):
        remote(wo.at[src * CORES + 1 - c], 3, opR.at[src], partner).wait_recv()

    tile = 2 * LANES

    def project(src, group, parts, first=False):
        wide = CORES * depth
        cols = pl.ds(pl.multiple_of(src * wide, wide), wide)
        for n in parts:
            at = slice(n * tile, (n + 1) * tile)
            part = jnp.dot(
                tok[:, :, cols].reshape(length, wide),
                wqkv[pl.ds(src * CORES, CORES), group, :, at].reshape(wide, tile),
                preferred_element_type=jnp.float32,
            )
            if first:
                acc[group, :, at] = part
            else:
                acc[group, :, at] += part

    def project_a(src, first=False):
        qp_copy(src, 0, mine=False).wait_recv()
        project(src, 0, (0, 1), first)

    def project_b(src, first=False, parts=(0, 1)):
        for n in parts:
            qp_copy(src, 1 + n, mine=False).wait_recv()
        project(src, 1, parts, first)

    def scores(group):
        for part in range(2):
            at = slice(part * LANES, (part + 1) * LANES)
            flat = acc[group, :, at].astype(jnp.bfloat16)
            turned = jnp.dot(flat, swap_ref[...], preferred_element_type=jnp.float32)
            qk[group, :, at] = (flat.astype(jnp.float32) * cos_ref[...] + turned * sin_ref[...]).astype(jnp.bfloat16)
        lane = lax.broadcasted_iota(jnp.int32, (length, LANES), 1)
        for inner in range(PAIR):
            query = qk[group, :, :LANES]
            query = jnp.where((lane // DK) == inner, query.astype(jnp.float32), 0.0).astype(jnp.bfloat16)
            for n in range(length // tile):
                at = slice(n * tile, (n + 1) * tile)
                part = lax.dot_general(
                    query, qk[group, at, LANES:], (((1,), (1,)), ((), ())), preferred_element_type=jnp.float32,
                )
                sc[inner, :, at] = (part * decay[group * PAIR + inner, :, at]).astype(jnp.bfloat16)

    def values(group):
        val[group] = acc[group, :, 2 * LANES :].astype(jnp.bfloat16)
        for inner in range(PAIR):
            head = group * PAIR + inner
            ret = jnp.dot(sc[inner], val[group, :, inner * DV : (inner + 1) * DV], preferred_element_type=jnp.float32)
            centred = ret - jnp.mean(ret, axis=-1, keepdims=True)
            variance = jnp.mean(centred * centred, axis=-1, keepdims=True)
            nown[head] = (centred * lax.rsqrt(variance + 1e-06)).astype(jnp.bfloat16)
            for to in (sd, sx, sy):
                n_copy(head, to).start()
            nrm[s, :, head * DV : (head + 1) * DV] = nown[head, pl.ds(pl.multiple_of(s * rows, rows), rows), :]

    def finish(units, first=False, last=False):
        for src, group in units:
            pl.when(src != s)(lambda: n_wait(group, src))
        for j in range(S):
            at = slice(j * oc, (j + 1) * oc)
            total = None if first else oacc[:, at]
            for src, group in units:
                part = jnp.dot(
                    nrm[src, :, group * wide_v : (group + 1) * wide_v], wo[src * CORES + group, j],
                    preferred_element_type=jnp.float32,
                )
                total = part if total is None else total + part
            if last:
                out_ref[:, at] = total.astype(out_ref.dtype)
            else:
                oacc[:, at] = total

    def on(where, fn, *args):
        pl.when(where)(lambda: fn(*args))

    both = (1, 2)
    local_wait(wo.at[pl.ds(0, S - 1), 0], 4)
    for j in range(S):
        op_copy(z, (s + j) % S).start()
    local_c[0].wait()
    decays(0)
    for half in range(2):
        t_copy(half, half, mine=False).wait_recv()
        r_copy(half).start()
    q_step(near, (0,))
    on(mid, q_step, second, (0,))
    o_step(o_first)
    for copy in local_c[1:]:
        copy.wait()
    t_copy(0, 1, mine=False).wait_recv()
    t_copy(1, 0, mine=False).wait_recv()
    for half in range(2):
        r_copy(half, mine=False).wait_recv()
    project_a(z, True)
    project_a(near)
    on(end, q_step, second, (0,))
    project_a(second)
    on(mid, q_step, third, (0,))
    on(mid, o_step, o_second)
    on(mid, own_q, both)
    o_relay(o_first)
    on(end, o_step, o_second)
    on(end, q_step, third, (0,))
    on(mid, q_step, near, both)
    project_a(third)
    scores(0)
    values(0)
    on(mid, o_step, third)
    decays(1)
    o_share(o_first)
    o_relay(o_second)
    on(mid, q_step, second, both)
    on(end, q_step, near, both)
    project_b(z, True)
    project_b(near)
    on(end, o_step, third)
    o_ready(z)
    o_ready(o_first)
    finish(((z, 0), (o_first, 0)), first=True)
    on(mid, q_step, third, both)
    o_share(o_second)
    o_ready(o_second)
    finish(((o_second, 0),))
    on(end, q_step, second, both)
    project_b(second)
    o_relay(third)
    on(end, q_step, third, (1,))
    project_b(third, parts=(0,))
    scores(1)
    on(end, q_step, third, (2,))
    project_b(third, parts=(1,))
    values(1)
    o_share(third)
    finish(((z, 1), (o_first, 1), (o_second, 1)))
    o_ready(third)
    finish(((third, 0), (third, 1)), last=True)

    def sent(ref, at):
        remote(ref, at, tR.at[0, 0], partner).wait_send()

    for where, count in ((mid, Z + 1), (end, 1)):
        @pl.when(where)
        def _():
            sent(wqkv.at[pl.ds(0, count)], 0)
            sent(wo.at[pl.ds(0, count), 0], 1)
    sent(wqkv.at[pl.ds(0, Z)], 2)
    sent(wo.at[pl.ds(0, Z)], 3)
    sent(wo.at[pl.ds(0, Z - 1), pl.ds(0, 2)], 4)
    sent(wo.at[pl.ds(0, Z - 1), 0], 5)
    sent(tok.at[pl.ds(0, S - 1)], 6)
    sent(nown.at[:, pl.ds(0, (S - 1) * rows)], 7)


def fused(S, Z, tokens, query_weight, key_weight, value_weight, output_weight, log_decay):
    rows, model = tokens.shape[1:]
    depth = query_weight.shape[0]
    heads = log_decay.shape[1]
    groups = heads // PAIR
    length = S * rows
    width = 2 * LANES + PAIR * DV
    oc = output_weight.shape[1] // S
    cosine, sine, swap = tables(length)
    anyplace = pl.BlockSpec(memory_space=pl.ANY)
    dma = pltpu.SemaphoreType.DMA
    bf, f32 = jnp.bfloat16, jnp.float32
    out = pl.pallas_call(
        functools.partial(layer_kernel, S, Z),
        out_shape=pltpu.VMEM((rows, output_weight.shape[1]), bf),
        in_specs=[anyplace] * 9,
        out_specs=pl.BlockSpec(memory_space=pltpu.VMEM),
        scratch_shapes=[
            pltpu.VMEM((S, rows, model), bf),
            pltpu.VMEM((Z * CORES, groups, depth, width), bf),
            pltpu.VMEM((Z * CORES, S, depth, oc), bf),
            pltpu.VMEM((groups, length, width), f32),
            pltpu.VMEM((heads, length, length), f32),
            pltpu.VMEM((groups, length, 2 * LANES), bf),
            pltpu.VMEM((groups, length, PAIR * DV), bf),
            pltpu.VMEM((PAIR, length, length), bf),
            pltpu.VMEM((heads, length, DV), bf),
            pltpu.VMEM((S, rows, heads * DV), bf),
            pltpu.VMEM((rows, S * oc), f32),
            pltpu.VMEM((length, LANES), f32), pltpu.VMEM((length, LANES), f32), pltpu.VMEM((LANES, LANES), bf),
            pltpu.SMEM((2, heads), f32),
            dma((9,)), dma((8,)), dma((2, 2)), dma((2,)), dma((Z, 3)), dma((Z, 3)),
            dma((Z, PIECES)), dma((2, Z)), dma((Z,)), dma((Z,)), dma((Z,)), dma((groups, S)),
        ],
        compiler_params=pltpu.CompilerParams(
            collective_id=0, has_side_effects=True, vmem_limit_bytes=56 * 1024 * 1024
        ),
    )(log_decay, cosine, sine, swap, tokens[0], query_weight, key_weight, value_weight, output_weight)
    return out[None]


def solution(mesh):
    S, D = mesh.shape["sp"], mesh.shape["dp"]
    Z = D // CORES

    def layer(tokens, query_weight, key_weight, value_weight, output_weight, log_decay):
        rows = tokens.shape[1]
        depth = query_weight.shape[0]
        heads = log_decay.shape[1]
        fits = (
            S == 4 and Z == 4 and D == CORES * Z and S * rows == BLOCK and heads == CORES * PAIR
            and PAIR * DV == depth and rows % 128 == 0
        )
        args = (tokens, query_weight, key_weight, value_weight, output_weight, log_decay)
        return fused(S, Z, *args) if fits else shards(*args)

    placed = (
        P("dp", "sp", None),
        P("dp", None),
        P("dp", None),
        P("dp", None),
        P("dp", None),
        P(None, "sp"),
    )
    return jax.shard_map(
        layer, mesh=mesh, in_specs=placed, out_specs=P("dp", "sp", None), check_vma=False
    )
```

```python
import functools

import numpy as np
import jax
import jax.numpy as jnp
from jax import lax
from jax.experimental import pallas as pl
from jax.experimental.pallas import tpu as pltpu
from jax.sharding import PartitionSpec as P

HEADS = 16
DK = 64
DV = 128
BLOCK = 512


exact_precision = lax.Precision.HIGHEST


def rotate(values_part, positions):
    half_dim = values_part.shape[-1] // 2
    frequency = 10000.0 ** (-jnp.arange(half_dim, dtype=jnp.float32) / half_dim)
    angles = positions[:, None] * frequency[None, :]
    cosine = jnp.cos(angles)[:, None, :]
    sine_part = jnp.sin(angles)[:, None, :]
    first = values_part[..., :half_dim]
    second = values_part[..., half_dim:]
    return jnp.concatenate(
        [first * cosine - second * sine_part, first * sine_part + second * cosine], axis=-1
    )


def retain(query, key_rows, value_rows, log_rate):
    length, heads, key_dim = query.shape
    value_dim = value_rows.shape[-1]
    count = length // BLOCK
    offsets = jnp.arange(BLOCK, dtype=jnp.float32)
    distance = offsets[:, None] - offsets[None, :]
    decay_inner = jnp.where(
        distance[None] >= 0.0,
        jnp.exp(log_rate[:, None, None] * jnp.maximum(distance, 0.0)[None]),
        0.0,
    )
    decay_query = jnp.exp((offsets[:, None] + 1.0) * log_rate[None, :])[:, :, None]
    decay_key = jnp.exp((BLOCK - 1.0 - offsets)[:, None] * log_rate[None, :])[:, :, None]
    decay_block = jnp.exp(BLOCK * log_rate)[:, None, None]

    def blocks(array):
        return array.reshape(count, BLOCK, heads, array.shape[-1])

    def advance(state, inputs):
        query_block, key_block, value_block = inputs
        inner = (
            jnp.einsum("ihd,jhd->hij", query_block, key_block, preferred_element_type=jnp.float32)
            * decay_inner
        )
        result = jnp.einsum(
            "hij,jhv->ihv",
            inner.astype(jnp.bfloat16),
            value_block,
            preferred_element_type=jnp.float32,
        )
        query_wide = query_block.astype(jnp.float32) * decay_query
        result = result + jnp.einsum("ihd,hdv->ihv", query_wide, state, precision=exact_precision)
        key_wide = key_block.astype(jnp.float32) * decay_key
        state = state * decay_block + jnp.einsum(
            "jhd,jhv->hdv", key_wide, value_block.astype(jnp.float32), precision=exact_precision
        )
        return (state, result)

    initial = jnp.zeros((heads, key_dim, value_dim), jnp.float32)
    final_state, outputs = lax.scan(
        advance, initial, (blocks(query), blocks(key_rows), blocks(value_rows))
    )
    return outputs.reshape(length, heads, value_dim)


def mechanism(stacked, log_decay):
    length = stacked.shape[0]
    widened = stacked[..., : 2 * DK].astype(jnp.float32)
    positions = jnp.arange(length, dtype=jnp.float32)
    query = rotate(widened[..., :DK], positions).astype(jnp.bfloat16)
    key_rows = rotate(widened[..., DK : 2 * DK], positions).astype(jnp.bfloat16)
    value_rows = stacked[..., 2 * DK :]
    forward = retain(query, key_rows, value_rows, log_decay[0])
    backward = retain(
        jnp.flip(query, 0), jnp.flip(key_rows, 0), jnp.flip(value_rows, 0), log_decay[1]
    )
    combined = forward + jnp.flip(backward, 0)
    average = jnp.mean(combined, axis=-1, keepdims=True)
    centred = combined - average
    variance = jnp.mean(centred * centred, axis=-1, keepdims=True)
    return (centred * lax.rsqrt(variance + 1e-06)).astype(jnp.bfloat16)


def shards(tokens, query_weight, key_weight, value_weight, output_weight, log_decay):
    rows = tokens[0]
    row_count = rows.shape[0]
    local_heads = log_decay.shape[1]
    first_head = lax.axis_index("sp") * local_heads
    own_slices = jnp.concatenate(
        [
            lax.dynamic_slice_in_dim(query_weight, first_head * DK, local_heads * DK, 1),
            lax.dynamic_slice_in_dim(key_weight, first_head * DK, local_heads * DK, 1),
            lax.dynamic_slice_in_dim(value_weight, first_head * DV, local_heads * DV, 1),
        ],
        axis=1,
    )
    own_whole = lax.all_gather(own_slices, "dp", axis=0, tiled=True)
    piece = lax.all_gather(rows, "sp", axis=0, tiled=True)
    count = piece.shape[0]
    product = jnp.dot(piece, own_whole, preferred_element_type=jnp.float32).astype(jnp.bfloat16)
    query_part = product[:, : local_heads * DK].reshape(count, local_heads, DK)
    key_part = product[:, local_heads * DK : 2 * local_heads * DK].reshape(count, local_heads, DK)
    value_part = product[:, 2 * local_heads * DK :].reshape(count, local_heads, DV)
    gathered = jnp.concatenate([query_part, key_part, value_part], axis=2)
    normed = mechanism(gathered, log_decay)
    by_token = lax.all_to_all(normed, "sp", split_axis=0, concat_axis=1, tiled=True).reshape(
        row_count, HEADS * DV
    )
    mixed = jnp.dot(
        by_token,
        lax.all_gather(output_weight, "dp", axis=0, tiled=True),
        preferred_element_type=jnp.float32,
    )
    return mixed.astype(jnp.bfloat16)[None]


MESH = pl.DeviceIdType.MESH
CORES = 2
PAIR = 2
PIECES = 2
LANES = PAIR * DK


def tables(length):
    half = DK // 2
    frequency = (10000.0 ** (-np.arange(half) / half)).astype(np.float32)
    angles = (np.arange(length, dtype=np.float32)[:, None] * frequency[None, :]).astype(np.float64)
    cosine = np.tile(np.cos(angles), (1, 4)).astype(np.float32)
    sine = np.tile(np.sin(angles), (1, 4)).astype(np.float32)
    swap = np.zeros((LANES, LANES), np.float32)
    for lane in range(LANES):
        if lane % DK < half:
            swap[lane + half, lane] = -1.0
        else:
            swap[lane - half, lane] = 1.0
    return jnp.asarray(cosine), jnp.asarray(sine), jnp.asarray(swap, jnp.bfloat16)


def layer_kernel(
    S, Z, rate_hbm, cos_hbm, sin_hbm, swap_hbm, x_ref, wq_ref, wk_ref, wv_ref, wo_ref, out_ref,
    tok, ftok, wqkv, wo, acc, decay, qk, val, sc, nown, fown, nrm, oacc, cos_ref, sin_ref, swap_ref, rate_ref,
    lsem, send, tR, rR, zR, fR, gR, qR, qpR, oR, xR, iR, jR, dR, opR, nR, hR,
):
    s = lax.axis_index("sp")
    d = lax.axis_index("dp")
    z, c = d // CORES, d % CORES
    rows, model = x_ref.shape
    length = S * rows
    depth = wq_ref.shape[0]
    heads = rate_hbm.shape[1]
    qc, vc = heads * DK, heads * DV
    wide_v = PAIR * DV
    oc = wo.shape[3]
    step_rows = depth // PIECES
    half_model = model // 2
    sx = s + 1 - 2 * (s % 2)
    sy = (s + 2) % 4
    sd = (sx + 2) % 4
    end = (z == 0) | (z == Z - 1)
    mid = jnp.logical_not(end)

    near, across, mirror = z + 1 - 2 * (z % 2), (z + 2) % Z, Z - 1 - z
    partner = {"dp": z * CORES + 1 - c}
    to_near, to_mirror = {"dp": near * CORES + c}, {"dp": mirror * CORES + c}

    def remote(src, send_at, recv, device, dst=None):
        return pltpu.make_async_remote_copy(
            src_ref=src, dst_ref=src if dst is None else dst, send_sem=send.at[send_at], recv_sem=recv,
            device_id=device, device_id_type=MESH,
        )

    def local(src, dst, at):
        return pltpu.make_async_copy(src, dst, lsem.at[at])

    def weight_copies(group):
        def part(ref, at, size, to):
            cols = pl.ds(pl.multiple_of(at + group * size, size), size)
            return local(ref.at[:, cols], wqkv.at[d, group, :, pl.ds(to, size)], group)

        return [
            part(wq_ref, s * qc, LANES, 0), part(wk_ref, s * qc, LANES, LANES),
            part(wv_ref, s * vc, wide_v, 2 * LANES),
        ]

    def quarter_copy(at, sem):
        return local(wo_ref.at[:, pl.ds(pl.multiple_of(at * oc, oc), oc)], wo.at[d, at], sem)

    def local_wait(ref, at):
        local(ref, ref, at).wait()

    local_c = [
        local(rate_hbm, rate_ref, 5), local(cos_hbm, cos_ref, 6),
        local(sin_hbm, sin_ref, 7), local(swap_hbm, swap_ref, 8),
    ]
    for copy in (
        weight_copies(0) + [local(x_ref, tok.at[s], 2), quarter_copy(s, 3)] + weight_copies(1)
        + local_c[:1] + [quarter_copy(at, 4) for at in (sd, sx, sy)] + local_c[1:]
    ):
        copy.start()

    barrier = pltpu.get_barrier_semaphore()

    def greet(device):
        pl.semaphore_signal(barrier, inc=1, device_id=device, device_id_type=MESH)

    greet(to_near)
    pl.when(mid)(lambda: greet(to_mirror))
    for other in range(1, S):
        greet({"sp": (s + other) % S})
    greet(partner)
    pl.when(mid)(lambda: pl.semaphore_wait(barrier, S + 2))
    pl.when(end)(lambda: pl.semaphore_wait(barrier, S + 1))

    def q_copy(src, group, device):
        return remote(wqkv.at[src * CORES + c, group], 0, qR.at[src, group], device)

    def qp_copy(src, group):
        return remote(wqkv.at[src * CORES + c, group], 2, qpR.at[src, group], partner)

    def qp_wait(src, group):
        remote(wqkv.at[src * CORES + 1 - c, group], 2, qpR.at[src, group], partner).wait_recv()

    def o_piece(block, quarter, piece):
        return wo.at[block, quarter, pl.ds(piece * step_rows, step_rows)]

    def o_copy(src, piece, device):
        return remote(o_piece(src * CORES + c, s, piece), 1, oR.at[src, piece], device)

    def x_copy(src, extra, device):
        return remote(wo.at[src * CORES + c, (sd, sx, sy)[extra]], 1, xR.at[src, extra], device)

    def op_copy(src, quarter):
        return remote(wo.at[src * CORES + c, quarter], 3, opR.at[src], partner)

    def o_ready(src):
        remote(wo.at[src * CORES + 1 - c], 3, opR.at[src], partner).wait_recv()

    def i_copy(axis, src, piece, recv):
        return remote(o_piece(src * CORES + c, s, piece), 4, recv, {"sp": sx if axis == 0 else sy})

    def d_copy(src, piece):
        to, quarter = (sy, sx) if piece == 0 else (sx, sy)
        return remote(o_piece(src * CORES + c, quarter, piece), 5, dR.at[src], {"sp": to})

    def half_ref(buffer, block, half):
        return buffer.at[block, :, pl.ds(half * half_model, half_model)]

    def t_copy(buffer, axis, half, at, recv):
        return remote(half_ref(buffer, s, half), at, recv.at[axis, half], {"sp": sx if axis == 0 else sy})

    def t_wait(buffer, axis, half, recv):
        remote(half_ref(buffer, sx if axis == 0 else sy, half), 6, recv.at[axis, half], {"sp": sx}).wait_recv()

    def r_copy(buffer, half, at, recv):
        to, block = (sy, sx) if half == 0 else (sx, sy)
        return remote(half_ref(buffer, block, half), at, recv.at[half], {"sp": to})

    def r_wait(buffer, half, recv):
        remote(half_ref(buffer, sd, half), 6, recv.at[half], {"sp": sx}).wait_recv()

    def z_copy(half):
        return remote(half_ref(tok, s, half), 10, zR.at[half], to_near, dst=half_ref(ftok, s, half))

    def n_copy(head, to):
        return remote(
            nown.at[head, pl.ds(pl.multiple_of(to * rows, rows), rows)], 7, nR.at[head // PAIR, s], {"sp": to},
            dst=nrm.at[s, :, pl.ds(head * DV, DV)],
        )

    def n_wait(group, j):
        ref = nrm.at[j, :, pl.ds(group * wide_v, wide_v)]
        remote(ref, 7, nR.at[group, j], {"sp": j}).wait_recv()

    def h_copy(inner, to):
        return remote(
            fown.at[inner, pl.ds(pl.multiple_of(to * rows, rows), rows)], 8, nR.at[1, s],
            {"sp": to, "dp": near * CORES + c}, dst=nrm.at[s, :, pl.ds((PAIR + inner) * DV, DV)],
        )

    def decays(group):
        for head in range(group * PAIR, (group + 1) * PAIR):
            fast, slow = rate_ref[0, head], rate_ref[1, head]

            @pl.loop(0, S)
            def _(j):
                at = lax.broadcasted_iota(jnp.int32, (rows, length), 0) + j * rows
                gap = (at - lax.broadcasted_iota(jnp.int32, (rows, length), 1)).astype(jnp.float32)
                weight = jnp.exp(jnp.where(gap >= 0.0, gap * fast, gap * (-slow)))
                decay[head, pl.ds(pl.multiple_of(j * rows, rows), rows), :] = jnp.where(gap == 0.0, 2.0, weight)

    tile = 2 * LANES

    def project(src, slot, buffer=tok, first=False):
        group = min(slot, 1)
        wide = CORES * depth
        cols = pl.ds(pl.multiple_of(src * wide, wide), wide)
        for n in range(2):
            at = slice(n * tile, (n + 1) * tile)
            part = jnp.dot(
                buffer[:, :, cols].reshape(length, wide),
                wqkv[pl.ds(src * CORES, CORES), group, :, at].reshape(wide, tile),
                preferred_element_type=jnp.float32,
            )
            if first:
                acc[slot, :, at] = part
            else:
                acc[slot, :, at] += part

    def scores(slot):
        for part in range(2):
            at = slice(part * LANES, (part + 1) * LANES)
            flat = acc[slot, :, at].astype(jnp.bfloat16)
            turned = jnp.dot(flat, swap_ref[...], preferred_element_type=jnp.float32)
            qk[:, at] = (flat.astype(jnp.float32) * cos_ref[...] + turned * sin_ref[...]).astype(jnp.bfloat16)
        lane = lax.broadcasted_iota(jnp.int32, (length, LANES), 1)
        for inner in range(PAIR):
            query = qk[:, :LANES]
            query = jnp.where((lane // DK) == inner, query.astype(jnp.float32), 0.0).astype(jnp.bfloat16)
            for n in range(length // tile):
                at = slice(n * tile, (n + 1) * tile)
                part = lax.dot_general(
                    query, qk[at, LANES:], (((1,), (1,)), ((), ())), preferred_element_type=jnp.float32,
                )
                sc[inner, :, at] = (part * decay[min(slot, 1) * PAIR + inner, :, at]).astype(jnp.bfloat16)

    def spread(head):
        for to in (sd, sx, sy):
            n_copy(head, to).start()
        nrm[s, :, head * DV : (head + 1) * DV] = nown[head, pl.ds(pl.multiple_of(s * rows, rows), rows), :]

    def values(slot):
        val[...] = acc[slot, :, 2 * LANES :].astype(jnp.bfloat16)
        for inner in range(PAIR):
            ret = jnp.dot(sc[inner], val[:, inner * DV : (inner + 1) * DV], preferred_element_type=jnp.float32)
            centred = ret - jnp.mean(ret, axis=-1, keepdims=True)
            variance = jnp.mean(centred * centred, axis=-1, keepdims=True)
            normed = (centred * lax.rsqrt(variance + 1e-06)).astype(jnp.bfloat16)
            if slot < 2:
                nown[slot * PAIR + inner] = normed
                spread(slot * PAIR + inner)
            else:
                fown[inner] = normed
                for to in (sd, sx, sy, s):
                    h_copy(inner, to).start()

    def retain(slot):
        scores(slot)
        values(slot)

    def finish(units, first=False, last=False, foreign=False):
        for src, group in units:
            if foreign:
                n_wait(group, src)
            else:
                pl.when(src != s)(lambda: n_wait(group, src))
        for j in range(S):
            at = slice(j * oc, (j + 1) * oc)
            total = None if first else oacc[:, at]
            for src, group in units:
                part = jnp.dot(
                    nrm[src, :, group * wide_v : (group + 1) * wide_v], wo[src * CORES + group, j],
                    preferred_element_type=jnp.float32,
                )
                total = part if total is None else total + part
            if last:
                out_ref[:, at] = total.astype(out_ref.dtype)
            else:
                oacc[:, at] = total

    def sent(ref, at):
        remote(ref, at, hR.at[0], partner).wait_send()

    def q_step(src, group, device=None):
        q_copy(src, group, to_near).wait_recv()
        if device is not None:
            q_copy(src, group, device).start()
        qp_copy(src, group).start()

    def project_in(src, slot, first=False):
        qp_wait(src, slot)
        project(src, slot, first=first)

    def tokens_out():
        local_wait(tok.at[s], 2)
        for half in range(2):
            t_copy(tok, 0, half, 6, tR).start()
            t_copy(tok, 1, 1 - half, 6, tR).start()

    def tokens_relay(buffer, at, recv, onward, halves=(0, 1)):
        for half in halves:
            t_wait(buffer, half, half, recv)
            r_copy(buffer, half, at, onward).start()

    def tokens_in(buffer, recv, onward):
        t_wait(buffer, 0, 1, recv)
        t_wait(buffer, 1, 0, recv)
        for half in range(2):
            r_wait(buffer, half, onward)

    def run_end():
        def o_step(src):
            for piece in range(PIECES):
                o_copy(src, piece, to_near).wait_recv()
                i_copy(piece, src, piece, iR.at[piece, src]).start()
                i_copy(1 - piece, src, piece, jR.at[src]).start()
            op_copy(src, s).start()

        def o_relay(src):
            for piece in range(PIECES):
                block = o_piece(src * CORES + c, sx if piece == 0 else sy, piece)
                remote(block, 4, iR.at[piece, src], {"sp": sx}).wait_recv()
                d_copy(src, piece).start()

        def o_share(src):
            remote(wo.at[src * CORES + c, sx], 4, jR.at[src], {"sp": sx}).wait_recv()
            op_copy(src, sx).start()
            op_copy(src, sy).start()
            remote(wo.at[src * CORES + c, sd], 5, dR.at[src], {"sp": sx}).wait_recv()
            op_copy(src, sd).start()

        local_wait(wqkv.at[d, 0], 0)
        q_copy(z, 0, to_near).start()
        tokens_out()
        qp_copy(z, 0).start()
        local_wait(wo.at[d, s], 3)
        for piece in range(PIECES):
            o_copy(z, piece, to_near).start()
        for half in range(2):
            z_copy(half).start()
        local_wait(wqkv.at[d, 1], 1)
        q_copy(z, 1, to_near).start()
        local_wait(wo.at[pl.ds(0, S - 1), 0], 4)
        for extra in range(S - 1):
            x_copy(z, extra, to_near).start()
        for at in (s, sd, sx, sy):
            op_copy(z, at).start()
        local_c[0].wait()
        decays(0)
        tokens_relay(tok, 6, tR, rR)
        q_step(near, 0)
        o_step(near)
        for copy in local_c[1:]:
            copy.wait()
        tokens_in(tok, tR, rR)
        project_in(z, 0, True)
        project_in(near, 0)
        q_step(across, 0)
        o_relay(near)
        project_in(across, 0)
        q_step(mirror, 0)
        project_in(mirror, 0)
        retain(0)
        o_share(near)
        o_step(mirror)
        o_ready(z)
        o_ready(near)
        finish(((z, 0), (near, 0)), first=True)
        o_step(across)
        o_relay(mirror)
        o_share(mirror)
        o_relay(across)
        o_ready(mirror)
        finish(((mirror, 0),))
        o_share(across)
        o_ready(across)
        finish(((across, 0),))
        finish(((z, 1), (near, 1), (mirror, 1), (across, 1)), last=True, foreign=True)
        sent(wqkv.at[pl.ds(0, 2), 0], 0)
        sent(wo.at[pl.ds(0, S), 0], 1)
        sent(wqkv.at[pl.ds(0, Z), 0], 2)
        sent(wo.at[pl.ds(0, Z)], 3)
        sent(wo.at[pl.ds(0, Z - 1), pl.ds(0, 2)], 4)
        sent(wo.at[pl.ds(0, Z - 1), 0], 5)
        sent(tok.at[0], 10)
        sent(nown.at[pl.ds(0, PAIR), pl.ds(0, (S - 1) * rows)], 7)

    def run_mid():
        def o_step(src, device):
            for piece in range(PIECES):
                o_copy(src, piece, device).wait_recv()
                o_copy(src, piece, device).start()
            op_copy(src, s).start()

        def o_send(src):
            for piece in range(PIECES):
                i_copy(0, src, piece, jR.at[src]).start()
                i_copy(1, src, piece, jR.at[src]).start()

        def x_step(src, extra, device=None):
            x_copy(src, extra, to_near).wait_recv()
            if device is not None:
                x_copy(src, extra, device).start()
            op_copy(src, (sd, sx, sy)[extra]).start()

        def o_share(src):
            remote(wo.at[src * CORES + c, pl.ds(0, 2)], 4, jR.at[src], {"sp": sx}).wait_recv()
            op_copy(src, sx).start()
            op_copy(src, sy).start()

        def foreign(half):
            remote(half_ref(ftok, s, half), 10, zR.at[half], to_near).wait_recv()
            t_copy(ftok, 0, half, 9, fR).start()
            t_copy(ftok, 1, half, 9, fR).start()

        local_wait(wqkv.at[d, 0], 0)
        q_copy(z, 0, to_near).start()
        q_copy(z, 0, to_mirror).start()
        tokens_out()
        qp_copy(z, 0).start()
        local_wait(wo.at[d, s], 3)
        for piece in range(PIECES):
            o_copy(z, piece, to_near).start()
        local_wait(wqkv.at[d, 1], 1)
        qp_copy(z, 1).start()
        local_wait(wo.at[pl.ds(0, S - 1), 0], 4)
        for at in (s, sd, sx, sy):
            op_copy(z, at).start()
        local_c[0].wait()
        decays(0)
        tokens_relay(tok, 6, tR, rR)
        q_step(near, 0, to_mirror)
        q_step(mirror, 0, to_near)
        o_step(near, to_mirror)
        q_copy(z, 1, to_mirror).start()
        for piece in range(PIECES):
            o_copy(z, piece, to_mirror).start()
        q_step(across, 0, to_near)
        for copy in local_c[1:]:
            copy.wait()
        tokens_in(tok, tR, rR)
        foreign(0)
        project_in(z, 0, True)
        project_in(near, 0)
        project_in(mirror, 0)
        o_step(across, to_near)
        project_in(across, 0)
        foreign(1)
        retain(0)
        q_step(mirror, 1)
        tokens_relay(ftok, 9, fR, gR, (0,))
        o_step(mirror, to_near)
        decays(1)
        project_in(z, 1, True)
        project_in(mirror, 1)
        tokens_relay(ftok, 9, fR, gR, (1,))
        q_step(near, 1, to_mirror)
        x_copy(z, 0, to_mirror).start()
        project_in(near, 1)
        o_ready(z)
        finish(((z, 0),), first=True)
        x_step(near, 0, to_mirror)
        q_step(across, 1)
        tokens_in(ftok, fR, gR)
        o_send(across)
        o_send(mirror)
        project(z, 2, ftok, True)
        project(near, 2, ftok)
        project(mirror, 2, ftok)
        qp_wait(across, 1)
        project(across, 2, ftok)
        retain(2)
        project(across, 1)
        retain(1)
        x_step(near, 1)
        x_step(mirror, 0)
        o_share(across)
        o_share(mirror)
        x_step(near, 2)
        o_ready(mirror)
        finish(((mirror, 0), (mirror, 1), (z, 1)))
        x_step(across, 0)
        o_ready(near)
        o_ready(across)
        finish(((across, 0), (across, 1), (near, 0), (near, 1)), last=True)
        sent(wqkv.at[pl.ds(0, 7), 0], 0)
        sent(wo.at[pl.ds(0, 7), 0], 1)
        sent(wqkv.at[pl.ds(0, Z)], 2)
        sent(wo.at[pl.ds(0, Z)], 3)
        sent(wo.at[pl.ds(0, 2), pl.ds(0, 2)], 4)
        sent(fown, 8)
        sent(nown.at[:, pl.ds(0, (S - 1) * rows)], 7)
        sent(ftok.at[pl.ds(0, S - 1)], 9)

    pl.when(end)(run_end)
    pl.when(mid)(run_mid)
    sent(tok.at[pl.ds(0, S - 1)], 6)


def fused(S, Z, tokens, query_weight, key_weight, value_weight, output_weight, log_decay):
    rows, model = tokens.shape[1:]
    depth = query_weight.shape[0]
    heads = log_decay.shape[1]
    groups = heads // PAIR
    length = S * rows
    width = 2 * LANES + PAIR * DV
    oc = output_weight.shape[1] // S
    cosine, sine, swap = tables(length)
    anyplace = pl.BlockSpec(memory_space=pl.ANY)
    dma = pltpu.SemaphoreType.DMA
    bf, f32 = jnp.bfloat16, jnp.float32
    out = pl.pallas_call(
        functools.partial(layer_kernel, S, Z),
        out_shape=pltpu.VMEM((rows, output_weight.shape[1]), bf),
        in_specs=[anyplace] * 9,
        out_specs=pl.BlockSpec(memory_space=pltpu.VMEM),
        scratch_shapes=[
            pltpu.VMEM((S, rows, model), bf),
            pltpu.VMEM((S, rows, model), bf),
            pltpu.VMEM((Z * CORES, groups, depth, width), bf),
            pltpu.VMEM((Z * CORES, S, depth, oc), bf),
            pltpu.VMEM((groups + 1, length, width), f32),
            pltpu.VMEM((heads, length, length), f32),
            pltpu.VMEM((length, 2 * LANES), bf),
            pltpu.VMEM((length, PAIR * DV), bf),
            pltpu.VMEM((PAIR, length, length), bf),
            pltpu.VMEM((heads, length, DV), bf),
            pltpu.VMEM((PAIR, length, DV), bf),
            pltpu.VMEM((S, rows, heads * DV), bf),
            pltpu.VMEM((rows, S * oc), f32),
            pltpu.VMEM((length, LANES), f32), pltpu.VMEM((length, LANES), f32), pltpu.VMEM((LANES, LANES), bf),
            pltpu.SMEM((2, heads), f32),
            dma((9,)), dma((11,)), dma((2, 2)), dma((2,)), dma((2,)), dma((2, 2)), dma((2,)),
            dma((Z, groups)), dma((Z, groups)), dma((Z, PIECES)), dma((Z, 3)),
            dma((2, Z)), dma((Z,)), dma((Z,)), dma((Z,)), dma((groups, S)), dma((PAIR,)),
        ],
        compiler_params=pltpu.CompilerParams(
            collective_id=0, has_side_effects=True, vmem_limit_bytes=56 * 1024 * 1024
        ),
    )(log_decay, cosine, sine, swap, tokens[0], query_weight, key_weight, value_weight, output_weight)
    return out[None]


def solution(mesh):
    S, D = mesh.shape["sp"], mesh.shape["dp"]
    Z = D // CORES

    def layer(tokens, query_weight, key_weight, value_weight, output_weight, log_decay):
        rows = tokens.shape[1]
        depth = query_weight.shape[0]
        heads = log_decay.shape[1]
        fits = (
            S == 4 and Z == 4 and D == CORES * Z and S * rows == BLOCK and heads == CORES * PAIR
            and PAIR * DV == depth and rows % 128 == 0
        )
        args = (tokens, query_weight, key_weight, value_weight, output_weight, log_decay)
        return fused(S, Z, *args) if fits else shards(*args)

    placed = (
        P("dp", "sp", None),
        P("dp", None),
        P("dp", None),
        P("dp", None),
        P("dp", None),
        P(None, "sp"),
    )
    return jax.shard_map(
        layer, mesh=mesh, in_specs=placed, out_specs=P("dp", "sp", None), check_vma=False
    )
```

```python
import functools

import numpy as np
import jax
import jax.numpy as jnp
from jax import lax
from jax.experimental import pallas as pl
from jax.experimental.pallas import tpu as pltpu
from jax.sharding import PartitionSpec as P

HEADS = 16
DK = 64
DV = 128
BLOCK = 512


exact_precision = lax.Precision.HIGHEST


def rotate(values_part, positions):
    half_dim = values_part.shape[-1] // 2
    frequency = 10000.0 ** (-jnp.arange(half_dim, dtype=jnp.float32) / half_dim)
    angles = positions[:, None] * frequency[None, :]
    cosine = jnp.cos(angles)[:, None, :]
    sine_part = jnp.sin(angles)[:, None, :]
    first = values_part[..., :half_dim]
    second = values_part[..., half_dim:]
    return jnp.concatenate(
        [first * cosine - second * sine_part, first * sine_part + second * cosine], axis=-1
    )


def retain(query, key_rows, value_rows, log_rate):
    length, heads, key_dim = query.shape
    value_dim = value_rows.shape[-1]
    count = length // BLOCK
    offsets = jnp.arange(BLOCK, dtype=jnp.float32)
    distance = offsets[:, None] - offsets[None, :]
    decay_inner = jnp.where(
        distance[None] >= 0.0,
        jnp.exp(log_rate[:, None, None] * jnp.maximum(distance, 0.0)[None]),
        0.0,
    )
    decay_query = jnp.exp((offsets[:, None] + 1.0) * log_rate[None, :])[:, :, None]
    decay_key = jnp.exp((BLOCK - 1.0 - offsets)[:, None] * log_rate[None, :])[:, :, None]
    decay_block = jnp.exp(BLOCK * log_rate)[:, None, None]

    def blocks(array):
        return array.reshape(count, BLOCK, heads, array.shape[-1])

    def advance(state, inputs):
        query_block, key_block, value_block = inputs
        inner = (
            jnp.einsum("ihd,jhd->hij", query_block, key_block, preferred_element_type=jnp.float32)
            * decay_inner
        )
        result = jnp.einsum(
            "hij,jhv->ihv",
            inner.astype(jnp.bfloat16),
            value_block,
            preferred_element_type=jnp.float32,
        )
        query_wide = query_block.astype(jnp.float32) * decay_query
        result = result + jnp.einsum("ihd,hdv->ihv", query_wide, state, precision=exact_precision)
        key_wide = key_block.astype(jnp.float32) * decay_key
        state = state * decay_block + jnp.einsum(
            "jhd,jhv->hdv", key_wide, value_block.astype(jnp.float32), precision=exact_precision
        )
        return (state, result)

    initial = jnp.zeros((heads, key_dim, value_dim), jnp.float32)
    final_state, outputs = lax.scan(
        advance, initial, (blocks(query), blocks(key_rows), blocks(value_rows))
    )
    return outputs.reshape(length, heads, value_dim)


def mechanism(stacked, log_decay):
    length = stacked.shape[0]
    widened = stacked[..., : 2 * DK].astype(jnp.float32)
    positions = jnp.arange(length, dtype=jnp.float32)
    query = rotate(widened[..., :DK], positions).astype(jnp.bfloat16)
    key_rows = rotate(widened[..., DK : 2 * DK], positions).astype(jnp.bfloat16)
    value_rows = stacked[..., 2 * DK :]
    forward = retain(query, key_rows, value_rows, log_decay[0])
    backward = retain(
        jnp.flip(query, 0), jnp.flip(key_rows, 0), jnp.flip(value_rows, 0), log_decay[1]
    )
    combined = forward + jnp.flip(backward, 0)
    average = jnp.mean(combined, axis=-1, keepdims=True)
    centred = combined - average
    variance = jnp.mean(centred * centred, axis=-1, keepdims=True)
    return (centred * lax.rsqrt(variance + 1e-06)).astype(jnp.bfloat16)


def shards(tokens, query_weight, key_weight, value_weight, output_weight, log_decay):
    rows = tokens[0]
    row_count = rows.shape[0]
    local_heads = log_decay.shape[1]
    first_head = lax.axis_index("sp") * local_heads
    own_slices = jnp.concatenate(
        [
            lax.dynamic_slice_in_dim(query_weight, first_head * DK, local_heads * DK, 1),
            lax.dynamic_slice_in_dim(key_weight, first_head * DK, local_heads * DK, 1),
            lax.dynamic_slice_in_dim(value_weight, first_head * DV, local_heads * DV, 1),
        ],
        axis=1,
    )
    own_whole = lax.all_gather(own_slices, "dp", axis=0, tiled=True)
    piece = lax.all_gather(rows, "sp", axis=0, tiled=True)
    count = piece.shape[0]
    product = jnp.dot(piece, own_whole, preferred_element_type=jnp.float32).astype(jnp.bfloat16)
    query_part = product[:, : local_heads * DK].reshape(count, local_heads, DK)
    key_part = product[:, local_heads * DK : 2 * local_heads * DK].reshape(count, local_heads, DK)
    value_part = product[:, 2 * local_heads * DK :].reshape(count, local_heads, DV)
    gathered = jnp.concatenate([query_part, key_part, value_part], axis=2)
    normed = mechanism(gathered, log_decay)
    by_token = lax.all_to_all(normed, "sp", split_axis=0, concat_axis=1, tiled=True).reshape(
        row_count, HEADS * DV
    )
    mixed = jnp.dot(
        by_token,
        lax.all_gather(output_weight, "dp", axis=0, tiled=True),
        preferred_element_type=jnp.float32,
    )
    return mixed.astype(jnp.bfloat16)[None]


MESH = pl.DeviceIdType.MESH
CORES = 2
PAIR = 2
PIECES = 2
LANES = PAIR * DK


def tables(length):
    half = DK // 2
    frequency = (10000.0 ** (-np.arange(half) / half)).astype(np.float32)
    angles = (np.arange(length, dtype=np.float32)[:, None] * frequency[None, :]).astype(np.float64)
    cosine = np.tile(np.cos(angles), (1, 4)).astype(np.float32)
    sine = np.tile(np.sin(angles), (1, 4)).astype(np.float32)
    swap = np.zeros((LANES, LANES), np.float32)
    for lane in range(LANES):
        if lane % DK < half:
            swap[lane + half, lane] = -1.0
        else:
            swap[lane - half, lane] = 1.0
    return jnp.asarray(cosine), jnp.asarray(sine), jnp.asarray(swap, jnp.bfloat16)


def layer_kernel(
    S, Z, rate_hbm, cos_hbm, sin_hbm, swap_hbm, x_ref, wq_ref, wk_ref, wv_ref, wo_ref, out_ref,
    tok, ftok, wqkv, wo, acc, decay, qk, val, sc, nown, fown, nrm, oacc, cos_ref, sin_ref, swap_ref, rate_ref,
    lsem, send, tR, rR, qR, qpR, oR, xR, iR, jR, dR, opR, nR,
):
    s = lax.axis_index("sp")
    d = lax.axis_index("dp")
    z, c = d // CORES, d % CORES
    rows, model = x_ref.shape
    length = S * rows
    depth = wq_ref.shape[0]
    heads = rate_hbm.shape[1]
    qc, vc = heads * DK, heads * DV
    wide_v = PAIR * DV
    oc = wo.shape[3]
    step_rows = depth // PIECES
    half_model = model // 2
    sx = s + 1 - 2 * (s % 2)
    sy = (s + 2) % 4
    sd = (sx + 2) % 4
    end = (z == 0) | (z == Z - 1)
    mid = jnp.logical_not(end)

    near, across, mirror = z + 1 - 2 * (z % 2), (z + 2) % Z, Z - 1 - z
    partner = {"dp": z * CORES + 1 - c}
    to_near, to_mirror = {"dp": near * CORES + c}, {"dp": mirror * CORES + c}

    def remote(src, send_at, recv, device, dst=None):
        return pltpu.make_async_remote_copy(
            src_ref=src, dst_ref=src if dst is None else dst, send_sem=send.at[send_at], recv_sem=recv,
            device_id=device, device_id_type=MESH,
        )

    def local(src, dst, at):
        return pltpu.make_async_copy(src, dst, lsem.at[at])

    def weight_copies(group):
        def part(ref, at, size, to):
            cols = pl.ds(pl.multiple_of(at + group * size, size), size)
            return local(ref.at[:, cols], wqkv.at[d, group, :, pl.ds(to, size)], group)

        return [
            part(wq_ref, s * qc, LANES, 0), part(wk_ref, s * qc, LANES, LANES),
            part(wv_ref, s * vc, wide_v, 2 * LANES),
        ]

    def quarter_copy(at, sem):
        return local(wo_ref.at[:, pl.ds(pl.multiple_of(at * oc, oc), oc)], wo.at[d, at], sem)

    def local_wait(ref, at):
        local(ref, ref, at).wait()

    local_c = [
        local(rate_hbm, rate_ref, 5), local(cos_hbm, cos_ref, 6),
        local(sin_hbm, sin_ref, 7), local(swap_hbm, swap_ref, 8),
    ]
    for copy in (
        weight_copies(0) + [local(x_ref, tok.at[s], 2), quarter_copy(s, 3)] + weight_copies(1)
        + local_c[:1] + [quarter_copy(at, 4) for at in (sd, sx, sy)] + local_c[1:]
    ):
        copy.start()

    barrier = pltpu.get_barrier_semaphore()

    def greet(device):
        pl.semaphore_signal(barrier, inc=1, device_id=device, device_id_type=MESH)

    greet(to_near)
    pl.when(mid)(lambda: greet(to_mirror))
    greet({"sp": sx})
    greet({"sp": sy})
    greet(partner)
    pl.when(mid)(lambda: pl.semaphore_wait(barrier, S + 1))
    pl.when(end)(lambda: pl.semaphore_wait(barrier, S))

    def q_copy(src, group, device):
        return remote(wqkv.at[src * CORES + c, group], 0, qR.at[src, group], device)

    def qp_copy(src, group):
        return remote(wqkv.at[src * CORES + c, group], 2, qpR.at[src, group], partner)

    def qp_wait(src, group):
        remote(wqkv.at[src * CORES + 1 - c, group], 2, qpR.at[src, group], partner).wait_recv()

    def o_piece(block, quarter, piece):
        return wo.at[block, quarter, pl.ds(piece * step_rows, step_rows)]

    def o_copy(src, piece, device):
        return remote(o_piece(src * CORES + c, s, piece), 1, oR.at[src, piece], device)

    def x_copy(src, extra, device):
        return remote(wo.at[src * CORES + c, (sd, sx, sy)[extra]], 1, dR.at[extra] if extra else xR.at[src], device)

    def op_copy(src, quarter):
        return remote(wo.at[src * CORES + c, quarter], 3, opR.at[src], partner)

    def o_ready(src):
        remote(wo.at[src * CORES + 1 - c], 3, opR.at[src], partner).wait_recv()

    def i_copy(axis, src, piece, recv):
        return remote(o_piece(src * CORES + c, s, piece), 4, recv, {"sp": sx if axis == 0 else sy})

    def d_copy(src, piece):
        to, quarter = (sy, sx) if piece == 0 else (sx, sy)
        return remote(o_piece(src * CORES + c, quarter, piece), 5, dR.at[src], {"sp": to})

    def half_ref(buffer, block, half):
        return buffer.at[block, :, pl.ds(half * half_model, half_model)]

    def t_copy(buffer, axis, half, at, recv):
        return remote(half_ref(buffer, s, half), at, recv.at[axis, half], {"sp": sx if axis == 0 else sy})

    def t_wait(buffer, axis, half, recv):
        remote(half_ref(buffer, sx if axis == 0 else sy, half), 6, recv.at[axis, half], {"sp": sx}).wait_recv()

    def r_copy(buffer, half, at):
        to, block = (sy, sx) if half == 0 else (sx, sy)
        return remote(half_ref(buffer, block, half), at, rR.at[half] if buffer is tok else iR.at[half, 2], {"sp": to})

    def r_wait(buffer, half):
        remote(half_ref(buffer, sd, half), 6, rR.at[half] if buffer is tok else iR.at[half, 2], {"sp": sx}).wait_recv()

    def z_copy(half):
        return remote(half_ref(tok, s, half), 10, iR.at[half, 3], to_near, dst=half_ref(ftok, s, half))

    def n_copy(head, to):
        return remote(
            nown.at[head, pl.ds(pl.multiple_of(to * rows, rows), rows)], 7, nR.at[head // PAIR, s], {"sp": to},
            dst=nrm.at[s, :, pl.ds(head * DV, DV)],
        )

    def n_wait(group, j):
        ref = nrm.at[j, :, pl.ds(group * wide_v, wide_v)]
        remote(ref, 7, nR.at[group, j], {"sp": j}).wait_recv()

    def h_copy(inner, to):
        return remote(
            fown.at[inner, pl.ds(pl.multiple_of(to * rows, rows), rows)], 8, nR.at[1, s],
            {"sp": to, "dp": near * CORES + c}, dst=nrm.at[s, :, pl.ds((PAIR + inner) * DV, DV)],
        )

    def decays(group):
        for head in range(group * PAIR, (group + 1) * PAIR):
            fast, slow = rate_ref[0, head], rate_ref[1, head]

            @pl.loop(0, S)
            def _(j):
                at = lax.broadcasted_iota(jnp.int32, (rows, length), 0) + j * rows
                gap = (at - lax.broadcasted_iota(jnp.int32, (rows, length), 1)).astype(jnp.float32)
                weight = jnp.exp(jnp.where(gap >= 0.0, gap * fast, gap * (-slow)))
                decay[head, pl.ds(pl.multiple_of(j * rows, rows), rows), :] = jnp.where(gap == 0.0, 2.0, weight)

    tile = 2 * LANES

    def project(src, slot, buffer=tok, first=False):
        group = min(slot, 1)
        wide = CORES * depth
        cols = pl.ds(pl.multiple_of(src * wide, wide), wide)
        for n in range(2):
            at = slice(n * tile, (n + 1) * tile)
            part = jnp.dot(
                buffer[:, :, cols].reshape(length, wide),
                wqkv[pl.ds(src * CORES, CORES), group, :, at].reshape(wide, tile),
                preferred_element_type=jnp.float32,
            )
            if first:
                acc[slot, :, at] = part
            else:
                acc[slot, :, at] += part

    def scores(slot):
        for part in range(2):
            at = slice(part * LANES, (part + 1) * LANES)
            flat = acc[slot, :, at].astype(jnp.bfloat16)
            turned = jnp.dot(flat, swap_ref[...], preferred_element_type=jnp.float32)
            qk[:, at] = (flat.astype(jnp.float32) * cos_ref[...] + turned * sin_ref[...]).astype(jnp.bfloat16)
        lane = lax.broadcasted_iota(jnp.int32, (length, LANES), 1)
        for inner in range(PAIR):
            query = qk[:, :LANES]
            query = jnp.where((lane // DK) == inner, query.astype(jnp.float32), 0.0).astype(jnp.bfloat16)
            for n in range(length // tile):
                at = slice(n * tile, (n + 1) * tile)
                part = lax.dot_general(
                    query, qk[at, LANES:], (((1,), (1,)), ((), ())), preferred_element_type=jnp.float32,
                )
                sc[inner, :, at] = (part * decay[min(slot, 1) * PAIR + inner, :, at]).astype(jnp.bfloat16)

    def spread(head):
        for to in (sd, sx, sy):
            n_copy(head, to).start()
        nrm[s, :, head * DV : (head + 1) * DV] = nown[head, pl.ds(pl.multiple_of(s * rows, rows), rows), :]

    def values(slot):
        val[...] = acc[slot, :, 2 * LANES :].astype(jnp.bfloat16)
        for inner in range(PAIR):
            ret = jnp.dot(sc[inner], val[:, inner * DV : (inner + 1) * DV], preferred_element_type=jnp.float32)
            centred = ret - jnp.mean(ret, axis=-1, keepdims=True)
            variance = jnp.mean(centred * centred, axis=-1, keepdims=True)
            normed = (centred * lax.rsqrt(variance + 1e-06)).astype(jnp.bfloat16)
            if slot < 2:
                nown[slot * PAIR + inner] = normed
                spread(slot * PAIR + inner)
            else:
                fown[inner] = normed
                for to in (sd, sx, sy, s):
                    h_copy(inner, to).start()

    def retain(slot):
        scores(slot)
        values(slot)

    def finish(units, first=False, last=False, foreign=False, waited=False):
        for src, group in units:
            if waited:
                continue
            if foreign:
                n_wait(group, src)
            else:
                pl.when(src != s)(lambda: n_wait(group, src))
        for j in range(S):
            at = slice(j * oc, (j + 1) * oc)
            total = None if first else oacc[:, at]
            for src, group in units:
                part = jnp.dot(
                    nrm[src, :, group * wide_v : (group + 1) * wide_v], wo[src * CORES + group, j],
                    preferred_element_type=jnp.float32,
                )
                total = part if total is None else total + part
            if last:
                out_ref[:, at] = total.astype(out_ref.dtype)
            else:
                oacc[:, at] = total

    def sent(ref, at):
        remote(ref, at, rR.at[0], partner).wait_send()

    def q_step(src, group, device=None):
        q_copy(src, group, to_near).wait_recv()
        if device is not None:
            q_copy(src, group, device).start()
        qp_copy(src, group).start()

    def project_in(src, slot, first=False):
        qp_wait(src, slot)
        project(src, slot, first=first)

    def tokens_out():
        local_wait(tok.at[s], 2)
        for half in range(2):
            t_copy(tok, 0, half, 6, tR).start()
            t_copy(tok, 1, 1 - half, 6, tR).start()

    def tokens_relay(buffer, at, recv, halves=(0, 1)):
        for half in halves:
            t_wait(buffer, half, half, recv)
            r_copy(buffer, half, at).start()

    def tokens_in(buffer, recv):
        t_wait(buffer, 0, 1, recv)
        t_wait(buffer, 1, 0, recv)
        for half in range(2):
            r_wait(buffer, half)

    def run_end():
        def o_step(src):
            for piece in range(PIECES):
                o_copy(src, piece, to_near).wait_recv()
                i_copy(piece, src, piece, iR.at[piece, src]).start()
                i_copy(1 - piece, src, piece, jR.at[src]).start()
            op_copy(src, s).start()

        def o_relay(src):
            for piece in range(PIECES):
                block = o_piece(src * CORES + c, sx if piece == 0 else sy, piece)
                remote(block, 4, iR.at[piece, src], {"sp": sx}).wait_recv()
                d_copy(src, piece).start()

        def o_share(src):
            remote(wo.at[src * CORES + c, sx], 4, jR.at[src], {"sp": sx}).wait_recv()
            op_copy(src, sx).start()
            op_copy(src, sy).start()
            remote(wo.at[src * CORES + c, sd], 5, dR.at[src], {"sp": sx}).wait_recv()
            op_copy(src, sd).start()

        local_wait(wqkv.at[d, 0], 0)
        q_copy(z, 0, to_near).start()
        tokens_out()
        qp_copy(z, 0).start()
        local_wait(wo.at[d, s], 3)
        for piece in range(PIECES):
            o_copy(z, piece, to_near).start()
        for half in range(2):
            z_copy(half).start()
        local_wait(wqkv.at[d, 1], 1)
        q_copy(z, 1, to_near).start()
        local_wait(wo.at[pl.ds(0, S - 1), 0], 4)
        for extra in range(S - 1):
            x_copy(z, extra, to_near).start()
        for at in (s, sd, sx, sy):
            op_copy(z, at).start()
        local_c[0].wait()
        decays(0)
        tokens_relay(tok, 6, tR)
        q_step(near, 0)
        o_step(near)
        for copy in local_c[1:]:
            copy.wait()
        tokens_in(tok, tR)
        project_in(z, 0, True)
        project_in(near, 0)
        q_step(across, 0)
        o_relay(near)
        project_in(across, 0)
        q_step(mirror, 0)
        project_in(mirror, 0)
        retain(0)
        o_share(near)
        o_step(mirror)
        o_ready(z)
        o_ready(near)
        finish(((z, 0), (near, 0)), first=True)
        o_step(across)
        o_relay(mirror)
        o_relay(across)
        o_share(mirror)
        o_ready(mirror)
        finish(((mirror, 0),))
        o_share(across)
        finish(((z, 1), (near, 1), (mirror, 1)), foreign=True)
        n_wait(1, across)
        o_ready(across)
        pl.when(across != s)(lambda: n_wait(0, across))
        finish(((across, 0), (across, 1)), last=True, waited=True)
        sent(wqkv.at[pl.ds(0, 2), 0], 0)
        sent(wo.at[pl.ds(0, S), 0], 1)
        sent(wqkv.at[pl.ds(0, Z), 0], 2)
        sent(wo.at[pl.ds(0, Z)], 3)
        sent(wo.at[pl.ds(0, Z - 1), pl.ds(0, 2)], 4)
        sent(wo.at[pl.ds(0, Z - 1), 0], 5)
        sent(tok.at[0], 10)
        sent(nown.at[pl.ds(0, PAIR), pl.ds(0, (S - 1) * rows)], 7)

    def run_mid():
        def o_step(src, device):
            for piece in range(PIECES):
                o_copy(src, piece, device).wait_recv()
                o_copy(src, piece, device).start()
            op_copy(src, s).start()

        def o_send(src):
            for piece in range(PIECES):
                i_copy(0, src, piece, jR.at[src]).start()
                i_copy(1, src, piece, jR.at[src]).start()

        def x_step(src, extra, device=None):
            x_copy(src, extra, to_near).wait_recv()
            if device is not None:
                x_copy(src, extra, device).start()
            op_copy(src, (sd, sx, sy)[extra]).start()

        def o_share(src):
            remote(wo.at[src * CORES + c, pl.ds(0, 2)], 4, jR.at[src], {"sp": sx}).wait_recv()
            op_copy(src, sx).start()
            op_copy(src, sy).start()

        def foreign(half):
            remote(half_ref(ftok, s, half), 10, iR.at[half, 3], to_near).wait_recv()
            t_copy(ftok, 0, half, 9, iR).start()
            t_copy(ftok, 1, half, 9, iR).start()

        local_wait(wqkv.at[d, 0], 0)
        q_copy(z, 0, to_near).start()
        q_copy(z, 0, to_mirror).start()
        tokens_out()
        qp_copy(z, 0).start()
        local_wait(wo.at[d, s], 3)
        for piece in range(PIECES):
            o_copy(z, piece, to_near).start()
        local_wait(wqkv.at[d, 1], 1)
        qp_copy(z, 1).start()
        local_wait(wo.at[pl.ds(0, S - 1), 0], 4)
        for at in (s, sd, sx, sy):
            op_copy(z, at).start()
        local_c[0].wait()
        decays(0)
        tokens_relay(tok, 6, tR)
        q_step(near, 0, to_mirror)
        q_step(mirror, 0, to_near)
        o_step(near, to_mirror)
        q_copy(z, 1, to_mirror).start()
        for piece in range(PIECES):
            o_copy(z, piece, to_mirror).start()
        q_step(across, 0, to_near)
        for copy in local_c[1:]:
            copy.wait()
        tokens_in(tok, tR)
        foreign(0)
        project_in(z, 0, True)
        project_in(near, 0)
        project_in(mirror, 0)
        o_step(across, to_near)
        project_in(across, 0)
        foreign(1)
        retain(0)
        q_step(mirror, 1)
        tokens_relay(ftok, 9, iR, (0,))
        o_step(mirror, to_near)
        decays(1)
        project_in(z, 1, True)
        project_in(mirror, 1)
        q_step(near, 1, to_mirror)
        x_copy(z, 0, to_mirror).start()
        tokens_relay(ftok, 9, iR, (1,))
        project_in(near, 1)
        o_ready(z)
        finish(((z, 0),), first=True)
        x_step(near, 0, to_mirror)
        q_step(across, 1)
        tokens_in(ftok, iR)
        o_send(across)
        o_send(mirror)
        project(z, 2, ftok, True)
        project(near, 2, ftok)
        project(mirror, 2, ftok)
        qp_wait(across, 1)
        project(across, 2, ftok)
        retain(2)
        project(across, 1)
        retain(1)
        x_step(near, 1)
        x_step(mirror, 0)
        o_share(across)
        x_step(near, 2)
        x_step(across, 0)
        o_share(mirror)
        o_ready(near)
        o_ready(across)
        finish(((near, 0), (across, 0)))
        finish(((z, 1), (near, 1), (across, 1)))
        o_ready(mirror)
        finish(((mirror, 0), (mirror, 1)), last=True)
        sent(wqkv.at[pl.ds(0, 7), 0], 0)
        sent(wo.at[pl.ds(0, 7), 0], 1)
        sent(wqkv.at[pl.ds(0, Z)], 2)
        sent(wo.at[pl.ds(0, Z)], 3)
        sent(wo.at[pl.ds(0, 2), pl.ds(0, 2)], 4)
        sent(fown, 8)
        sent(nown.at[:, pl.ds(0, (S - 1) * rows)], 7)
        sent(ftok.at[pl.ds(0, S - 1)], 9)

    pl.when(end)(run_end)
    pl.when(mid)(run_mid)
    sent(tok.at[pl.ds(0, S - 1)], 6)


def fused(S, Z, tokens, query_weight, key_weight, value_weight, output_weight, log_decay):
    rows, model = tokens.shape[1:]
    depth = query_weight.shape[0]
    heads = log_decay.shape[1]
    groups = heads // PAIR
    length = S * rows
    width = 2 * LANES + PAIR * DV
    oc = output_weight.shape[1] // S
    cosine, sine, swap = tables(length)
    anyplace = pl.BlockSpec(memory_space=pl.ANY)
    dma = pltpu.SemaphoreType.DMA
    bf, f32 = jnp.bfloat16, jnp.float32
    out = pl.pallas_call(
        functools.partial(layer_kernel, S, Z),
        out_shape=pltpu.VMEM((rows, output_weight.shape[1]), bf),
        in_specs=[anyplace] * 9,
        out_specs=pl.BlockSpec(memory_space=pltpu.VMEM),
        scratch_shapes=[
            pltpu.VMEM((S, rows, model), bf),
            pltpu.VMEM((S, rows, model), bf),
            pltpu.VMEM((Z * CORES, groups, depth, width), bf),
            pltpu.VMEM((Z * CORES, S, depth, oc), bf),
            pltpu.VMEM((groups + 1, length, width), f32),
            pltpu.VMEM((heads, length, length), f32),
            pltpu.VMEM((length, 2 * LANES), bf),
            pltpu.VMEM((length, PAIR * DV), bf),
            pltpu.VMEM((PAIR, length, length), bf),
            pltpu.VMEM((heads, length, DV), bf),
            pltpu.VMEM((PAIR, length, DV), bf),
            pltpu.VMEM((S, rows, heads * DV), bf),
            pltpu.VMEM((rows, S * oc), f32),
            pltpu.VMEM((length, LANES), f32), pltpu.VMEM((length, LANES), f32), pltpu.VMEM((LANES, LANES), bf),
            pltpu.SMEM((2, heads), f32),
            dma((9,)), dma((11,)), dma((2, 2)), dma((2,)),
            dma((Z, groups)), dma((Z, groups)), dma((Z, PIECES)), dma((Z,)),
            dma((2, Z)), dma((Z,)), dma((Z,)), dma((Z,)), dma((groups, S)),
        ],
        compiler_params=pltpu.CompilerParams(
            collective_id=0, has_side_effects=True, vmem_limit_bytes=56 * 1024 * 1024
        ),
    )(log_decay, cosine, sine, swap, tokens[0], query_weight, key_weight, value_weight, output_weight)
    return out[None]


def solution(mesh):
    S, D = mesh.shape["sp"], mesh.shape["dp"]
    Z = D // CORES

    def layer(tokens, query_weight, key_weight, value_weight, output_weight, log_decay):
        rows = tokens.shape[1]
        depth = query_weight.shape[0]
        heads = log_decay.shape[1]
        fits = (
            S == 4 and Z == 4 and D == CORES * Z and S * rows == BLOCK and heads == CORES * PAIR
            and PAIR * DV == depth and rows % 128 == 0
        )
        args = (tokens, query_weight, key_weight, value_weight, output_weight, log_decay)
        return fused(S, Z, *args) if fits else shards(*args)

    placed = (
        P("dp", "sp", None),
        P("dp", None),
        P("dp", None),
        P("dp", None),
        P("dp", None),
        P(None, "sp"),
    )
    return jax.shard_map(
        layer, mesh=mesh, in_specs=placed, out_specs=P("dp", "sp", None), check_vma=False
    )
```
